32 devices in a mesh: fs: 4 (over y, x), tp: 8 (over z, core).
Axes of the slice: x: 2, y: 2, z: 4, core: 2. Of those that a mesh axis runs over, the one named last changes fastest.
Arguments:
- tokens: bfloat16 [512, 4096], P('fs', 'tp'), may hold values from -6 to 6
- expert_ids: int32 [512, 8], P('fs'), may hold values from 0 to 63, all different within a row; in each aligned block of 128 rows (0 to 127, 128 to 255, ...) at most 32 rows name the same one
- affinity: float32 [512, 8], P('fs'), may hold values from 0.05 to 1
- norm_gain: float32 [4096], P('fs'), may hold values from 0.1 to 1.9
- gate_train: float32 [64, 512, 4096], P(None, 'tp', 'fs'), may hold values from -0.09375 to 0.09375
- up_train: float32 [64, 512, 4096], P(None, 'tp', 'fs'), may hold values from -0.09375 to 0.09375
- down_train: float32 [64, 512, 4096], P(None, 'fs', 'tp'), may hold values from -0.25 to 0.25
- shared_gate_train: float32 [512, 4096], P('tp', 'fs'), may hold values from -0.09375 to 0.09375
- shared_up_train: float32 [512, 4096], P('tp', 'fs'), may hold values from -0.09375 to 0.09375
- shared_down_train: float32 [512, 4096], P('fs', 'tp'), may hold values from -0.25 to 0.25
Outputs:
- mixed: bfloat16 [512, 4096], P('fs', 'tp')
- gate_serve: bfloat16 [64, 512, 4096], P('fs', 'tp')
- up_serve: bfloat16 [64, 512, 4096], P('fs', 'tp')
- down_serve: bfloat16 [64, 512, 4096], P('fs', None, 'tp')
- shared_gate_serve: bfloat16 [512, 4096], P('tp')
- shared_up_serve: bfloat16 [512, 4096], P('tp')
- shared_down_serve: bfloat16 [512, 4096], P(None, 'tp')
The draws below stay inside these ranges and needn't reach their ends.
Inputs may be any that keep to these rules, and one draw needn't show every extreme that they name: `expert_ids`: each row names 8 different experts. In each aligned block of 128 rows (the tokens of one index of fs) no expert is named by more than 32 rows, a bound that some block reaches.
All inputs are finite; a program needn't handle non-finite values.
Results may differ from the reference program's by a relative error of at most 0.019.
Values may be sent and summed in bfloat16 or wider, within the bound.
A program may use at most 192 MiB of HBM per device.

```python
import math
import jax
import jax.numpy as jnp
import numpy as np
from jax import lax

D = 4096
H = 512
EXPERTS = 64
K = 8
TOK = 128
CAP = 32
TOKENS = 512
N_FS = 4


def block_scale(own_key, dims, cuts, smallest, high):
    level = 1.0
    for dim, shards_of in cuts:
        heights = jax.random.uniform(jax.random.fold_in(jax.random.fold_in(own_key, 6), dim), (shards_of,), jnp.float32, smallest / len(cuts), high / len(cuts))
        level = level * jnp.repeat(jnp.exp(heights), dims[dim] // shards_of).reshape((-1,) + (1,) * (len(dims) - 1 - dim))
    return level


def assign_block(stream_key, own, number, rows, amount, top, reach, lean):
    order = jax.random.permutation(stream_key, amount)
    packed, usual = shares(amount, rows * top, reach, lean, True), shares(amount, rows * top, reach, lean, False)
    places = jnp.arange(amount)

    def named(tallies, rotation):
        used = int((tallies > 0).sum())
        fixed = max(1, used // 4)
        moved = fixed + (places - fixed + rotation * (used - fixed)) % max(1, amount - fixed)
        return jnp.zeros((amount,), jnp.int32).at[order[jnp.where(places < fixed, places, moved)]].set(jnp.asarray(tallies, jnp.int32))

    tallies = jnp.where(number % 4 == 0, named(packed, number // 4), named(usual, number - number // 4 - 1))
    mixed = jax.random.permutation(jax.random.fold_in(own, 3), amount)
    giver, taker = mixed[0:amount // 2 * 2:2], mixed[1:amount // 2 * 2:2]
    slack = jnp.minimum(tallies[giver] - 1, reach - tallies[taker]) // 2
    slack = jnp.where((giver == order[0]) | (taker == order[0]) | (tallies[taker] == 0), 0, jnp.maximum(slack, 0))
    moved = jax.random.randint(jax.random.fold_in(own, 4), (amount // 2,), 0, 1 << 20) % (slack + 1)
    tallies = tallies.at[giver].add(-moved).at[taker].add(moved)
    items = jnp.searchsorted(jnp.cumsum(tallies), jnp.arange(rows * top), side="right").astype(jnp.int32)
    table = items.reshape(top, rows).T
    table = table[jax.random.permutation(jax.random.fold_in(own, 1), rows)]
    rotation = jax.random.randint(jax.random.fold_in(own, 2), (rows, 1), 0, top)
    return jnp.take_along_axis(table, (jnp.arange(top)[None, :] + rotation) % top, axis=1)


def shares(count, total, limit, lean, full):
    portions = [(1 << 20) // math.isqrt(rank ** lean) + 1 for rank in range(1, count + 1)]
    largest = limit if full else min(limit, max(-(-total // count), total * portions[0] // sum(portions)))
    least = 1 if total - largest >= count - 1 else 0
    holding, spare = [largest] + [least] * (count - 1), total - largest - least * (count - 1)
    while spare > 0:
        free = [i for i in range(1, count) if holding[i] < largest] or [i for i in range(1, count) if holding[i] < limit]
        whole, left = sum([portions[i] for i in free]), spare
        for i in free:
            more = min(limit - holding[i], max(1, left * portions[i] // whole), spare)
            holding[i] = holding[i] + more
            spare = spare - more
    return np.array(holding)


def bell_draw(key, extent, scale, limit, pieces=(), kind=jnp.bfloat16):
    result = scale * jax.random.normal(key, extent, jnp.float32)
    if pieces:
        result = result * block_scale(key, extent, pieces, -0.22, 0.18)
    return jnp.clip(result, -limit, limit).astype(kind)


def setup_inputs(seed: int = 0) -> dict:
    seeds = jax.random.split(jax.random.key(seed), 11)
    tokens = bell_draw(seeds[0], (TOKENS, D), 1.0, 6.0, ((0, 4), (1, 8)))
    expert_ids_keys = jax.random.split(jax.random.fold_in(seeds[1], 1), TOKENS // TOK)
    expert_ids_turns = jax.random.permutation(jax.random.fold_in(seeds[1], 3), TOKENS // TOK)
    expert_ids = jax.vmap(lambda own, number: assign_block(jax.random.fold_in(seeds[1], 2), own, number, TOK, EXPERTS, K, CAP, 1))(expert_ids_keys, expert_ids_turns).reshape((TOKENS, K))
    affinity = jnp.clip(0.05 + 0.95 * jax.random.uniform(seeds[2], (TOKENS, K), jnp.float32) ** block_scale(seeds[2], (TOKENS, K), ((0, 4),), -0.2, 0.2), 0.05, 1.0)
    norm_gain = jnp.clip(1.0 + 0.18 * jax.random.normal(seeds[3], (D,), jnp.float32), 0.1, 1.9)
    gate_train = bell_draw(seeds[4], (EXPERTS, H, D), D ** -0.5, 0.09375, ((1, 8), (2, 4)), jnp.float32)
    up_train = bell_draw(seeds[5], (EXPERTS, H, D), D ** -0.5, 0.09375, ((1, 8), (2, 4)), jnp.float32)
    down_train = bell_draw(seeds[6], (EXPERTS, H, D), H ** -0.5, 0.25, ((1, 4), (2, 8)), jnp.float32)
    shared_gate_train = bell_draw(seeds[7], (H, D), D ** -0.5, 0.09375, ((0, 8), (1, 4)), jnp.float32)
    shared_up_train = bell_draw(seeds[8], (H, D), D ** -0.5, 0.09375, ((0, 8), (1, 4)), jnp.float32)
    shared_down_train = bell_draw(seeds[9], (H, D), H ** -0.5, 0.25, ((0, 4), (1, 8)), jnp.float32)
    return {"tokens": tokens, "expert_ids": expert_ids, "affinity": affinity, "norm_gain": norm_gain, "gate_train": gate_train, "up_train": up_train, "down_train": down_train, "shared_gate_train": shared_gate_train, "shared_up_train": shared_up_train, "shared_down_train": shared_down_train}


norm_eps = 1e-06
routed_scale = 2.5

def reference(tokens, expert_ids, affinity, norm_gain, gate_train, up_train, down_train, shared_gate_train, shared_up_train, shared_down_train):
    gain_cols = norm_gain[None, None, :]
    gate_serve = (gate_train * gain_cols).astype(jnp.bfloat16)
    up_serve = (up_train * gain_cols).astype(jnp.bfloat16)
    down_serve = down_train.astype(jnp.bfloat16)
    shared_gate_serve = (shared_gate_train * norm_gain[None, :]).astype(jnp.bfloat16)
    shared_up_serve = (shared_up_train * norm_gain[None, :]).astype(jnp.bfloat16)
    shared_down_serve = shared_down_train.astype(jnp.bfloat16)
    widened = tokens.astype(jnp.float32)
    inverse_rms = lax.rsqrt(lax.optimization_barrier(jnp.mean(widened * widened, axis=1)) + norm_eps)
    shared_gate = jnp.dot(tokens, shared_gate_serve.T, preferred_element_type=jnp.float32) * inverse_rms[:, None]
    shared_up = jnp.dot(tokens, shared_up_serve.T, preferred_element_type=jnp.float32) * inverse_rms[:, None]
    shared_hidden = (jax.nn.silu(shared_gate) * shared_up).astype(jnp.bfloat16)
    shared_out = jnp.dot(shared_hidden, shared_down_serve, preferred_element_type=jnp.float32)
    ids = expert_ids.reshape(N_FS, TOK * K)
    onehot = (ids[:, :, None] == jnp.arange(EXPERTS, dtype=jnp.int32)[None, None, :]).astype(jnp.int32)
    slot_index = lax.optimization_barrier(jnp.sum((jnp.cumsum(onehot, axis=1) - onehot) * onehot, axis=2))
    block_index = jnp.arange(N_FS, dtype=jnp.int32)[:, None]
    position = (ids * (N_FS * CAP) + block_index * CAP + slot_index).reshape(-1).astype(jnp.int32)
    token_of = jnp.repeat(jnp.arange(TOKENS, dtype=jnp.int32), K)
    rows = jnp.zeros((EXPERTS * N_FS * CAP, D), jnp.bfloat16).at[position].set(tokens[token_of])
    scales = jnp.zeros((EXPERTS * N_FS * CAP,), jnp.float32).at[position].set(inverse_rms[token_of])

    def one_expert(operands):
        rows_e, scale_e, gate_w, up_w, down_w = operands
        gate_pre = jnp.dot(rows_e, gate_w.T, preferred_element_type=jnp.float32) * scale_e[:, None]
        up_pre = jnp.dot(rows_e, up_w.T, preferred_element_type=jnp.float32) * scale_e[:, None]
        hidden = (jax.nn.silu(gate_pre) * up_pre).astype(jnp.bfloat16)
        return jnp.dot(hidden, down_w, preferred_element_type=jnp.float32).astype(jnp.bfloat16)
    outputs = lax.map(one_expert, (rows.reshape(EXPERTS, N_FS * CAP, D), scales.reshape(EXPERTS, N_FS * CAP), gate_serve, up_serve, down_serve))
    picked = outputs.reshape(EXPERTS * N_FS * CAP, D)[position].reshape(TOKENS, K, D).astype(jnp.float32)
    route_weight = routed_scale * affinity / lax.optimization_barrier(jnp.sum(affinity, axis=1, keepdims=True))
    routed = lax.optimization_barrier(jnp.sum(picked * route_weight[:, :, None], axis=1))
    mixed = (shared_out + routed).astype(jnp.bfloat16)
    return (mixed, gate_serve, up_serve, down_serve, shared_gate_serve, shared_up_serve, shared_down_serve)
```

```python
import functools

import jax
import jax.numpy as jnp
from jax import lax
from jax.experimental import pallas as pl
from jax.experimental.pallas import tpu as pltpu
from jax.sharding import PartitionSpec as P

MESH = pl.DeviceIdType.MESH

norm_eps = 1e-06
routed_scale = 2.5
vmem_bytes = 66900000


def nt_dot(a, b):
    return lax.dot_general(a, b, (((1,), (1,)), ((), ())), preferred_element_type=jnp.float32)


def silu_mul(acc, scale):
    half = acc.shape[1] // 2
    gate = acc[:, :half] * scale
    up = acc[:, half:] * scale
    return gate / (1.0 + jnp.exp(-gate)) * up


def moe_kernel(cfg, *refs):
    n, ntp, group, slots, cols, ge = cfg
    (ids_ref, aff_ref, gain_ref, tok_ref, gate_ref, up_ref, down_ref, sg_ref, su_ref, sd_ref) = refs[:10]
    (mixed_ref, gout, uout, dout, sgo, suo, sdo) = refs[10:17]
    (idv, affv, gainv, rbuf, rland, routes, x, inv, fbuf, sbuf, dfb, dsb) = refs[17:29]
    (gfb, ufb, sfb, gsb, usb, ssb, hid, hids, acc, own, part, landed) = refs[29:41]
    (isem, lsem, tsem, osem, zs, zr, gss, grs, dss, drs, mss, mrs, hs, hr, qs, qr, cs, cr) = refs[41:]

    me = lax.axis_index("fs")
    tp = lax.axis_index("tp")
    dest = [lax.rem(me + k, n) for k in range(n)]
    origin = [lax.rem(me + n - k, n) for k in range(n)]
    nz = ntp // 2
    partner = tp + 1 - 2 * lax.rem(tp, 2)
    zdest = [lax.rem(tp + 2 * k, ntp) for k in range(nz)]
    zorigin = [lax.rem(tp + ntp - 2 * k, ntp) for k in range(nz)]
    porigin = [lax.rem(partner + ntp - 2 * k, ntp) for k in range(nz)]

    rows = tok_ref.shape[0]
    total_rows = n * rows
    topk = ids_ref.shape[0]
    le, hl, d = gout.shape
    dl = d // n
    hd = down_ref.shape[1]
    hidden = hd * n
    cl = down_ref.shape[2]
    pairs = le // group
    gl = group * hl
    cw = cl // cols
    neg = le // ge
    chunks = cols * neg
    order = list(range(1, n)) + [0]

    def at(first, size):
        return pl.ds(pl.multiple_of(first, size), size)

    def to_fs(k):
        return {"fs": dest[k]}

    smalls = [(sg_ref, gfb, gsb, sgo), (su_ref, ufb, usb, suo), (sd_ref, sfb, ssb, sdo)]
    early = [(ids_ref, idv), (aff_ref, affv), (gain_ref, gainv)] + [(s, f) for s, f, _, _ in smalls]

    def early_load(i):
        return pltpu.make_async_copy(early[i][0], early[i][1], isem.at[i])

    weights = [gate_ref, up_ref]
    wouts = [gout, uout]

    def load(w, j, k):
        return pltpu.make_async_copy(
            weights[w].at[pl.ds(dest[k] * le + j * group, group)], fbuf.at[k], lsem.at[0, k]
        )

    def dload(c, k):
        cb, eg = c // neg, lax.rem(c, neg)
        return pltpu.make_async_copy(
            down_ref.at[pl.ds(dest[k] * le + eg * ge, ge), :, at(cb * cw, cw)], dfb.at[k], lsem.at[1, k]
        )

    def own_tokens():
        return pltpu.make_async_copy(tok_ref, x.at[at(me * rows, rows), at(tp * cl, cl)], osem)

    for i in range(len(early)):
        early_load(i).start()
    for k in order:
        load(0, 0, k).start()
    own_tokens().start()

    barrier = pltpu.get_barrier_semaphore()
    for k in range(1, n):
        pl.semaphore_signal(barrier, inc=1, device_id=to_fs(k), device_id_type=MESH)
    for k in range(1, nz):
        pl.semaphore_signal(barrier, inc=1, device_id={"tp": zdest[k]}, device_id_type=MESH)
    pl.semaphore_signal(barrier, inc=1, device_id={"tp": partner}, device_id_type=MESH)
    pl.semaphore_wait(barrier, n - 1 + nz)

    def token_copy(k, source):
        return pltpu.make_async_remote_copy(
            src_ref=tok_ref,
            dst_ref=x.at[at(source * rows, rows), at(tp * cl, cl)],
            send_sem=tsem.at[0, k],
            recv_sem=tsem.at[1, k],
            device_id=to_fs(k),
            device_id_type=MESH,
        )

    def route_copy(k, source):
        return pltpu.make_async_remote_copy(
            src_ref=rbuf,
            dst_ref=rland.at[source],
            send_sem=tsem.at[2, k],
            recv_sem=tsem.at[3, k],
            device_id=to_fs(k),
            device_id_type=MESH,
        )

    for k in range(1, n):
        token_copy(k, me).start()

    for i in range(3):
        early_load(i).wait()
    affinity = affv[...]
    route = jnp.concatenate(
        [idv[...].astype(jnp.float32), routed_scale * affinity / jnp.sum(affinity, axis=0, keepdims=True)], axis=0
    )
    rbuf[...] = route
    rland[me] = route

    def weight_copy(w, k, slot, j, source):
        return pltpu.make_async_remote_copy(
            src_ref=sbuf.at[w, k - 1, slot],
            dst_ref=wouts[w].at[pl.ds(j * group, group), :, at(source * dl, dl)],
            send_sem=gss.at[w, k - 1, slot],
            recv_sem=grs.at[w, k - 1, j],
            device_id=to_fs(k),
            device_id_type=MESH,
        )

    def produce(j):
        slot = lax.rem(j, slots)
        for w in range(2):
            pending = None
            for k in order:
                load(w, j, k).wait()
                for c in range(group):
                    value = (fbuf[k, c] * gainv[...]).astype(jnp.bfloat16)
                    if k == 0:
                        wouts[w][j * group + c, :, at(me * dl, dl)] = value
                    else:
                        sbuf[w, k - 1, slot, c] = value
                if w == 0:
                    load(1, j, k).start()
                else:

                    @pl.when(j + 1 < pairs)
                    def _():
                        load(0, j + 1, k).start()

                if pending is not None:
                    weight_copy(w, pending, slot, j, me).start()
                pending = k

    def first(j, carry):
        produce(j)
        return carry

    lax.fori_loop(0, slots, first, 0)

    for k in range(1, n):
        route_copy(k, me).start()

    def small_place(i, who):
        ref = smalls[i][3]
        if i == 2:
            return ref.at[at(who * hd, hd), :]
        return ref.at[:, at(who * dl, dl)]

    def small_copy(i, k, source):
        return pltpu.make_async_remote_copy(
            src_ref=smalls[i][2],
            dst_ref=small_place(i, source),
            send_sem=mss.at[i, k - 1],
            recv_sem=mrs.at[i, k - 1],
            device_id=to_fs(k),
            device_id_type=MESH,
        )

    for i in range(3):
        early_load(3 + i).wait()
        value = smalls[i][1][...]
        if i < 2:
            value = value * gainv[...]
        value = value.astype(jnp.bfloat16)
        smalls[i][2][...] = value
        small_place(i, me)[...] = value
    for i in range(3):
        for k in range(1, n):
            small_copy(i, k, me).start()

    def z_copy(view, send, recv, index, slot, to):
        return pltpu.make_async_remote_copy(
            src_ref=view(slot),
            dst_ref=view(slot),
            send_sem=send(index),
            recv_sem=recv(index),
            device_id={"tp": to},
            device_id_type=MESH,
        )

    def z_send(view, send, recv):
        for k in range(1, nz):
            z_copy(view, send, recv, k, tp, zdest[k]).start()
        z_copy(view, send, recv, 0, tp, partner).start()

    def z_relay(view, send, recv):
        for k in range(1, nz):
            z_copy(view, send, recv, k, zorigin[k], zdest[k]).wait_recv()
            z_copy(view, send, recv, nz - 1 + k, zorigin[k], partner).start()

    def z_finish(view, send, recv):
        z_copy(view, send, recv, 0, partner, partner).wait_recv()
        for k in range(1, nz):
            z_copy(view, send, recv, nz - 1 + k, porigin[k], partner).wait_recv()

    def z_sent(view, send, recv):
        for k in range(2 * nz - 1):
            z_copy(view, send, recv, k, tp, partner).wait_send()

    def pick(sems):
        return lambda i: sems.at[i]

    def token_view(slot):
        return x.at[:, at(slot * cl, cl)]

    own_tokens().wait()
    for k in range(1, n):
        token_copy(k, origin[k]).wait_recv()
    z_send(token_view, pick(zs), pick(zr))
    for k in range(1, n):
        route_copy(k, origin[k]).wait_recv()
    for f in range(n):
        routes[f * rows : (f + 1) * rows, : 2 * topk] = rland[f].T
    z_relay(token_view, pick(zs), pick(zr))
    z_finish(token_view, pick(zs), pick(zr))

    block = min(512, total_rows)

    def norms(i, carry):
        part_rows = at(i * 128, 128)
        sums = jnp.zeros((128, 1), jnp.float32)
        for c in range(0, d, 512):
            v = x[part_rows, c : c + 512].astype(jnp.float32)
            sums = sums + jnp.sum(v * v, axis=1, keepdims=True)
        inv[part_rows, :] = jnp.broadcast_to(lax.rsqrt(sums / d + norm_eps), (128, inv.shape[1]))
        return carry

    lax.fori_loop(0, total_rows // 128, norms, 0)

    def down_place(c, who):
        cb, eg = c // neg, lax.rem(c, neg)
        return dout.at[pl.ds(eg * ge, ge), at(who * hd, hd), at(cb * cw, cw)]

    def down_copy(k, c, source):
        return pltpu.make_async_remote_copy(
            src_ref=dsb.at[k - 1, c],
            dst_ref=down_place(c, source),
            send_sem=dss.at[k - 1, c],
            recv_sem=drs.at[k - 1, c],
            device_id=to_fs(k),
            device_id_type=MESH,
        )

    def produce_down():
        for k in order:
            dload(0, k).start()

        def step(c, carry):
            pending = None
            for k in order:
                dload(c, k).wait()
                for e in range(ge):
                    value = dfb[k, e].astype(jnp.bfloat16)
                    if k == 0:
                        cb, eg = c // neg, lax.rem(c, neg)
                        dout[eg * ge + e, at(me * hd, hd), at(cb * cw, cw)] = value
                    else:
                        dsb[k - 1, c, e] = value

                @pl.when(c + 1 < chunks)
                def _():
                    dload(c + 1, k).start()

                if pending is not None:
                    down_copy(pending, c, me).start()
                pending = k
            return carry

        lax.fori_loop(0, chunks, step, 0)

    def hid_view(i):
        return lambda slot: hid.at[slot, i]

    def hid_sem(sems, i):
        return lambda k: sems.at[i, k]

    def hid_args(i):
        return hid_view(i), hid_sem(hs, i), hid_sem(hr, i)

    def consume(i, carry):
        for w in range(2):
            for k in range(1, n):
                weight_copy(w, k, 0, i, origin[k]).wait_recv()
        w_all = jnp.concatenate(
            [gout[pl.ds(i * group, group)].reshape(gl, d), uout[pl.ds(i * group, group)].reshape(gl, d)], axis=0
        )

        def rows_step(r, c):
            rs = at(r * block, block)
            h = silu_mul(nt_dot(x[rs, :], w_all), inv[rs, :gl])
            lane = lax.broadcasted_iota(jnp.int32, h.shape, 1)
            expert = (me * le + group * i + lane // hl).astype(jnp.float32)
            weight = jnp.zeros(h.shape, jnp.float32)
            for k in range(topk):
                weight = weight + jnp.where(
                    routes[rs, k : k + 1] == expert, routes[rs, topk + k : topk + k + 1], 0.0
                )
            hid[tp, i, rs, :] = (h * weight).astype(jnp.bfloat16)
            return c

        if total_rows == block:
            rows_step(0, 0)
        else:
            lax.fori_loop(0, total_rows // block, rows_step, 0)

        @pl.when(i > 0)
        def _():
            z_relay(*hid_args(i - 1))

        z_send(*hid_args(i))

        @pl.when(i + slots < pairs)
        def _():
            for w in range(2):
                for k in range(1, n):
                    weight_copy(w, k, lax.rem(i, slots), i, me).wait_send()
            produce(i + slots)

        if pairs > slots:

            @pl.when(i == pairs - slots - 1)
            def _():
                produce_down()

        return carry

    if pairs == slots:
        produce_down()
    lax.fori_loop(0, pairs, consume, 0)
    z_relay(*hid_args(pairs - 1))

    def shared_view(slot):
        return hids.at[slot]

    shared_args = (shared_view, pick(qs), pick(qr))
    for i in range(3):
        for k in range(1, n):
            small_copy(i, k, origin[k]).wait_recv()
    mine = at(me * rows, rows)
    h = silu_mul(nt_dot(x[mine, :], jnp.concatenate([sgo[...], suo[...]], axis=0)), inv[mine, :hl])
    wide = jnp.concatenate([h] * group, axis=1)
    lane = lax.broadcasted_iota(jnp.int32, wide.shape, 1)
    hids[tp] = jnp.where(lane // hl == lax.rem(tp, group), wide, 0.0).astype(jnp.bfloat16)

    def finish(i, carry):
        z_finish(*hid_args(i))
        return carry

    lax.fori_loop(0, pairs, finish, 0)
    z_send(*shared_args)
    z_relay(*shared_args)
    z_finish(*shared_args)
    blocks = []
    for q in range(ntp // group):
        blocks.append(functools.reduce(jnp.add, [hids[q * group + g] for g in range(group)]))
    shared = jnp.dot(jnp.concatenate(blocks, axis=1), sdo[...], preferred_element_type=jnp.float32)
    for cb in range(cols):
        own[cb] = shared[:, cb * cw : (cb + 1) * cw]

    def part_copy(k, cb, who):
        return pltpu.make_async_remote_copy(
            src_ref=part.at[cb, at(who * rows, rows)],
            dst_ref=landed.at[cb, k - 1],
            send_sem=cs.at[cb, k - 1],
            recv_sem=cr.at[cb, k - 1],
            device_id=to_fs(k),
            device_id_type=MESH,
        )

    per = ge // group

    def down_step(c, carry):
        cb, eg = c // neg, lax.rem(c, neg)
        for k in range(1, n):
            down_copy(k, c, origin[k]).wait_recv()
        left, right = [], []
        for p in range(per):
            pair = eg * per + p
            for s in range(ntp):
                left.append(hid.at[s, pair])
                right.append(
                    dout[pl.ds(pair * group, group), s * hl : (s + 1) * hl, at(cb * cw, cw)].reshape(gl, cw)
                )
        down = jnp.concatenate(right, axis=0)

        def rows_step(r, q):
            rs = at(r * block, block)
            lhs = jnp.concatenate([ref[rs, :] for ref in left], axis=1)
            total = jnp.dot(lhs, down, preferred_element_type=jnp.float32)

            @pl.when(eg == 0)
            def _():
                acc[rs, :] = total

            @pl.when(eg > 0)
            def _():
                acc[rs, :] += total

            return q

        if total_rows == block:
            rows_step(0, 0)
        else:
            lax.fori_loop(0, total_rows // block, rows_step, 0)

        @pl.when(eg == neg - 1)
        def _():
            part[cb] = acc[...].astype(jnp.bfloat16)
            own[cb] += acc[mine, :]
            for k in range(1, n):
                part_copy(k, cb, dest[k]).start()

        return carry

    lax.fori_loop(0, chunks, down_step, 0)

    for k in range(1, n):
        token_copy(k, me).wait_send()
        route_copy(k, me).wait_send()
        for i in range(3):
            small_copy(i, k, me).wait_send()
    z_sent(token_view, pick(zs), pick(zr))
    z_sent(*shared_args)

    def sent(i, carry):
        z_sent(*hid_args(i))
        return carry

    lax.fori_loop(0, pairs, sent, 0)

    def weights_sent(j, carry):
        for w in range(2):
            for k in range(1, n):
                weight_copy(w, k, lax.rem(j, slots), j, me).wait_send()
        return carry

    lax.fori_loop(pairs - slots, pairs, weights_sent, 0)

    def down_sent(c, carry):
        for k in range(1, n):
            down_copy(k, c, me).wait_send()
        return carry

    lax.fori_loop(0, chunks, down_sent, 0)

    for cb in range(cols):
        result = own[cb]
        for k in range(1, n):
            part_copy(k, cb, dest[k]).wait()
            result = result + landed[cb, k - 1].astype(jnp.float32)
        mixed_ref[:, cb * cw : (cb + 1) * cw] = result.astype(mixed_ref.dtype)


def moe_call(n, ntp, args):
    ids, aff, gain, tokens, gate, up, down, sg, su, sd = args
    bf16, f32 = jnp.bfloat16, jnp.float32
    experts, hl, dl = gate.shape
    _, hd, cl = down.shape
    rows = tokens.shape[0]
    topk = ids.shape[0]
    le, d, hidden, total = experts // n, dl * n, hd * n, rows * n
    group = min(le, max(1, 128 // hl))
    pairs = le // group
    slots = min(4, pairs)
    cols = 2 if cl % 256 == 0 else 1
    cw = cl // cols
    ge = group * (2 if pairs % 2 == 0 else 1)
    chunks = cols * (le // ge)
    gl = group * hl
    nz = ntp // 2
    vm, dma = pltpu.VMEM, pltpu.SemaphoreType.DMA
    outs = [
        ((rows, cl), bf16),
        ((le, hl, d), bf16),
        ((le, hl, d), bf16),
        ((le, hidden, cl), bf16),
        ((hl, d), bf16),
        ((hl, d), bf16),
        ((hidden, cl), bf16),
    ]
    pinned = sum(functools.reduce(lambda a, b: a * b, s) * 2 for s, _ in outs)
    hbm = pl.BlockSpec(memory_space=pltpu.HBM)
    args = [pltpu.with_memory_space_constraint(a, pltpu.HBM) for a in args]
    results = pl.pallas_call(
        functools.partial(moe_kernel, (n, ntp, group, slots, cols, ge)),
        out_shape=tuple(vm(s, t) for s, t in outs),
        in_specs=[hbm] * len(args),
        out_specs=(pl.BlockSpec(memory_space=vm),) * len(outs),
        scratch_shapes=[
            vm(ids.shape, ids.dtype),
            vm(aff.shape, f32),
            vm(gain.shape, f32),
            vm((2 * topk, rows), f32),
            vm((n, 2 * topk, rows), f32),
            vm((total, 128), f32),
            vm((total, d), bf16),
            vm((total, 128), f32),
            vm((n, group, hl, dl), f32),
            vm((2, n - 1, slots, group, hl, dl), bf16),
            vm((n, ge, hd, cw), f32),
            vm((n - 1, chunks, ge, hd, cw), bf16),
            vm(sg.shape, f32),
            vm(su.shape, f32),
            vm(sd.shape, f32),
            vm(sg.shape, bf16),
            vm(su.shape, bf16),
            vm(sd.shape, bf16),
            vm((ntp, pairs, total, gl), bf16),
            vm((ntp, rows, gl), bf16),
            vm((total, cw), f32),
            vm((cols, rows, cw), f32),
            vm((cols, total, cw), bf16),
            vm((cols, n - 1, rows, cw), bf16),
            dma((6,)),
            dma((2, n)),
            dma((4, n)),
            dma,
            dma((2 * nz - 1,)),
            dma((2 * nz - 1,)),
            dma((2, n - 1, slots)),
            dma((2, n - 1, pairs)),
            dma((n - 1, chunks)),
            dma((n - 1, chunks)),
            dma((3, n - 1)),
            dma((3, n - 1)),
            dma((pairs, 2 * nz - 1)),
            dma((pairs, 2 * nz - 1)),
            dma((2 * nz - 1,)),
            dma((2 * nz - 1,)),
            dma((cols, n - 1)),
            dma((cols, n - 1)),
        ],
        compiler_params=pltpu.CompilerParams(
            collective_id=0, has_side_effects=True, vmem_limit_bytes=min(60 * 1024 * 1024, vmem_bytes - pinned)
        ),
        cost_estimate=pl.CostEstimate(flops=6 * total * d * hl * le, bytes_accessed=40 * gate.size, transcendentals=0),
    )(*args)

    def write(*refs):
        count = len(outs)
        sem = refs[-1]
        copies = [pltpu.make_async_copy(refs[i], refs[count + i], sem.at[i]) for i in range(count)]
        for c in copies:
            c.start()
        for c in copies:
            c.wait()

    return pl.pallas_call(
        write,
        out_shape=tuple(jax.ShapeDtypeStruct(s, t) for s, t in outs),
        in_specs=[pl.BlockSpec(memory_space=vm)] * len(outs),
        out_specs=(hbm,) * len(outs),
        scratch_shapes=[dma((len(outs),))],
        compiler_params=pltpu.CompilerParams(vmem_limit_bytes=1024 * 1024),
        cost_estimate=pl.CostEstimate(flops=0, bytes_accessed=pinned, transcendentals=0),
    )(*results)


def body(
    n,
    ntp,
    tokens,
    expert_ids,
    affinity,
    norm_gain,
    gate_train,
    up_train,
    down_train,
    shared_gate_train,
    shared_up_train,
    shared_down_train,
):
    return moe_call(
        n,
        ntp,
        [
            expert_ids.T,
            affinity.T,
            norm_gain[None, :],
            tokens,
            gate_train,
            up_train,
            down_train,
            shared_gate_train,
            shared_up_train,
            shared_down_train,
        ],
    )


def solution(mesh):
    return jax.shard_map(
        functools.partial(body, mesh.shape["fs"], mesh.shape["tp"]),
        mesh=mesh,
        in_specs=(
            P("fs", "tp"),
            P("fs", None),
            P("fs", None),
            P("fs"),
            P(None, "tp", "fs"),
            P(None, "tp", "fs"),
            P(None, "fs", "tp"),
            P("tp", "fs"),
            P("tp", "fs"),
            P("fs", "tp"),
        ),
        out_specs=(
            P("fs", "tp"),
            P("fs", "tp", None),
            P("fs", "tp", None),
            P("fs", None, "tp"),
            P("tp", None),
            P("tp", None),
            P(None, "tp"),
        ),
        check_vma=False,
    )
```

```python
import functools

import jax
import jax.numpy as jnp
from jax import lax
from jax.experimental import pallas as pl
from jax.experimental.pallas import tpu as pltpu
from jax.sharding import PartitionSpec as P

MESH = pl.DeviceIdType.MESH

norm_eps = 1e-06
routed_scale = 2.5
vmem_bytes = 66900000


def nt_dot(a, b):
    return lax.dot_general(a, b, (((1,), (1,)), ((), ())), preferred_element_type=jnp.float32)


def mate(me, k, n):
    if n & (n - 1):
        return lax.rem(me + k, n)
    other, bit = 0, 1
    while bit < n:
        other = other + bit * lax.rem(lax.div(me, bit) + k // bit, 2)
        bit *= 2
    return other


def mate_origin(me, k, n):
    return lax.rem(me + n - k, n) if n & (n - 1) else mate(me, k, n)


def mate_pairs(k, n):
    return [(i, (i + k) % n if n & (n - 1) else i ^ k) for i in range(n)]


def silu_mul(acc, scale):
    half = acc.shape[1] // 2
    gate = acc[:, :half] * scale
    up = acc[:, half:] * scale
    return gate / (1.0 + jnp.exp(-gate)) * up


def moe_kernel(cfg, *refs):
    n, ntp, group, slots, cols, ge = cfg
    (ids_ref, aff_ref, gain_ref, tok_ref, gate_ref, up_ref, down_ref, sg_ref, su_ref, sd_ref) = refs[:10]
    (gout, uout, dout, sgo, suo, own) = refs[10:16]
    lasts = refs[16 : 15 + n]
    refs = refs[15 + n :]
    (idv, affv, gainv, rbuf, rland, routes, x, inv, fbuf, sbuf, dfb, dsb) = refs[:12]
    (gfb, ufb, sfb, ssb, hid, acc, part, landed) = refs[12:20]
    (isem, lsem, tsem, osem, zs, zr, gss, grs, dss, drs, mss, mrs, hs, hr, cs, cr, rsem) = refs[20:]

    me = lax.axis_index("fs")
    tp = lax.axis_index("tp")
    dest = [lax.rem(me + k, n) for k in range(n)]
    origin = [lax.rem(me + n - k, n) for k in range(n)]
    nz = ntp // 2
    partner = tp + 1 - 2 * lax.rem(tp, 2)
    zdest = [lax.rem(tp + 2 * k, ntp) for k in range(nz)]
    zorigin = [lax.rem(tp + ntp - 2 * k, ntp) for k in range(nz)]
    porigin = [lax.rem(partner + ntp - 2 * k, ntp) for k in range(nz)]

    rows = tok_ref.shape[0]
    total_rows = n * rows
    topk = ids_ref.shape[0]
    le, hl, d = gout.shape
    dl = d // n
    hd = down_ref.shape[1]
    sources = hd // hl
    cl = down_ref.shape[2]
    pairs = le // group
    gl = group * hl
    cw = cl // cols
    neg = le // ge
    chunks = cols * neg
    order = list(range(1, n)) + [0]

    def at(first, size):
        return pl.ds(pl.multiple_of(first, size), size)

    def to_fs(k):
        return {"fs": dest[k]}

    smalls = [(gfb, sgo), (ufb, suo)]
    early = [(ids_ref, idv), (aff_ref, affv), (gain_ref, gainv), (sg_ref, gfb), (su_ref, ufb), (sd_ref, sfb)]

    def early_load(i):
        return pltpu.make_async_copy(early[i][0], early[i][1], isem.at[i])

    weights = [gate_ref, up_ref]
    wouts = [gout, uout]

    def load(w, j, k):
        return pltpu.make_async_copy(
            weights[w].at[pl.ds(dest[k] * le + j * group, group)], fbuf.at[k], lsem.at[0, k]
        )

    def dload(c, k):
        cb, eg = c // neg, lax.rem(c, neg)
        return pltpu.make_async_copy(
            down_ref.at[pl.ds(dest[k] * le + eg * ge, ge), :, at(cb * cw, cw)], dfb.at[k], lsem.at[1, k]
        )

    def own_tokens():
        return pltpu.make_async_copy(tok_ref, x.at[at(me * rows, rows), at(tp * cl, cl)], osem)

    for i in range(len(early)):
        early_load(i).start()
    for k in order:
        load(0, 0, k).start()
    own_tokens().start()

    barrier = pltpu.get_barrier_semaphore()
    for k in range(1, n):
        pl.semaphore_signal(barrier, inc=1, device_id=to_fs(k), device_id_type=MESH)
    for k in range(1, nz):
        pl.semaphore_signal(barrier, inc=1, device_id={"tp": zdest[k]}, device_id_type=MESH)
    pl.semaphore_signal(barrier, inc=1, device_id={"tp": partner}, device_id_type=MESH)
    pl.semaphore_wait(barrier, n - 1 + nz)

    relay = n == 4
    near = [mate(me, k, n) for k in (1, 2)] if relay else []
    far = mate(me, 3, n) if relay else None

    def fs_copy(src, dst, sems, index, to):
        return pltpu.make_async_remote_copy(
            src_ref=src,
            dst_ref=dst,
            send_sem=sems[0](index),
            recv_sem=sems[1](index),
            device_id={"fs": to},
            device_id_type=MESH,
        )

    def gather_start(src, view, sems):
        for i, to in enumerate(near if relay else dest[1:]):
            fs_copy(src, view(me, None), sems, i, to).start()

    def gather_relay(view, sems):
        if relay:
            for i in range(2):
                whole = view(near[i], None)
                fs_copy(whole, whole, sems, i, near[i]).wait_recv()
                half = view(near[i], i)
                fs_copy(half, half, sems, 2 + i, near[1 - i]).start()

    def gather_wait(view, sems):
        if relay:
            for i in range(2):
                half = view(far, i)
                fs_copy(half, half, sems, 2 + i, near[1 - i]).wait_recv()
        else:
            for k in range(1, n):
                whole = view(origin[k], None)
                fs_copy(whole, whole, sems, k - 1, dest[k]).wait_recv()

    def gather_sent(view, sems):
        for i in range(2 if relay else n - 1):
            whole = view(me, None)
            fs_copy(whole, whole, sems, i, dest[1]).wait_send()
        if relay:
            for i in range(2):
                half = view(near[i], i)
                fs_copy(half, half, sems, 2 + i, near[1 - i]).wait_send()

    def token_place(who, half):
        size = rows if half is None else rows // 2
        return x.at[at(who * rows + (half or 0) * size, size), at(tp * cl, cl)]

    token_sems = (lambda i: tsem.at[0, i], lambda i: tsem.at[1, i])

    def route_copy(k, source):
        return pltpu.make_async_remote_copy(
            src_ref=rbuf,
            dst_ref=rland.at[source],
            send_sem=rsem.at[0, k],
            recv_sem=rsem.at[1, k],
            device_id=to_fs(k),
            device_id_type=MESH,
        )

    gather_start(tok_ref, token_place, token_sems)

    for i in range(3):
        early_load(i).wait()
    affinity = affv[...]
    route = jnp.concatenate(
        [idv[...].astype(jnp.float32), routed_scale * affinity / jnp.sum(affinity, axis=0, keepdims=True)], axis=0
    )
    rbuf[...] = route
    rland[me] = route

    def weight_copy(w, k, slot, j, source):
        return pltpu.make_async_remote_copy(
            src_ref=sbuf.at[w, k - 1, slot],
            dst_ref=wouts[w].at[pl.ds(j * group, group), :, at(source * dl, dl)],
            send_sem=gss.at[w, k - 1, slot],
            recv_sem=grs.at[w, k - 1, j],
            device_id=to_fs(k),
            device_id_type=MESH,
        )

    def produce(j):
        slot = lax.rem(j, slots)
        for w in range(2):
            pending = None
            for k in order:
                load(w, j, k).wait()
                for c in range(group):
                    value = (fbuf[k, c] * gainv[...]).astype(jnp.bfloat16)
                    if k == 0:
                        wouts[w][j * group + c, :, at(me * dl, dl)] = value
                    else:
                        sbuf[w, k - 1, slot, c] = value
                if w == 0:
                    load(1, j, k).start()
                else:

                    @pl.when(j + 1 < pairs)
                    def _():
                        load(0, j + 1, k).start()

                if pending is not None:
                    weight_copy(w, pending, slot, j, me).start()
                pending = k

    def first(j, carry):
        produce(j)

        @pl.when(j == 0)
        def _():
            gather_relay(token_place, token_sems)

        return carry

    lax.fori_loop(0, slots, first, 0)

    for k in range(1, n):
        route_copy(k, me).start()

    def small_place(i):
        def view(who, half):
            size = hl if half is None else hl // 2
            return smalls[i][1].at[pl.ds((half or 0) * size, size), at(who * dl, dl)]

        return view

    small_sems = [(lambda k, i=i: mss.at[i, k], lambda k, i=i: mrs.at[i, k]) for i in range(2)]
    for i in range(2):
        early_load(3 + i).wait()
        smalls[i][1][:, at(me * dl, dl)] = (smalls[i][0][...] * gainv[...]).astype(jnp.bfloat16)
    for i in range(2):
        gather_start(small_place(i)(me, None), small_place(i), small_sems[i])
    early_load(5).wait()
    ssb[...] = sfb[...].astype(jnp.bfloat16)

    def z_copy(view, send, recv, index, slot, to):
        return pltpu.make_async_remote_copy(
            src_ref=view(slot),
            dst_ref=view(slot),
            send_sem=send(index),
            recv_sem=recv(index),
            device_id={"tp": to},
            device_id_type=MESH,
        )

    def z_send(view, send, recv):
        for k in range(1, nz):
            z_copy(view, send, recv, k, tp, zdest[k]).start()
        z_copy(view, send, recv, 0, tp, partner).start()

    def z_relay(view, send, recv):
        for k in range(1, nz):
            z_copy(view, send, recv, k, zorigin[k], zdest[k]).wait_recv()
            z_copy(view, send, recv, nz - 1 + k, zorigin[k], partner).start()

    def z_finish(view, send, recv):
        z_copy(view, send, recv, 0, partner, partner).wait_recv()
        for k in range(1, nz):
            z_copy(view, send, recv, nz - 1 + k, porigin[k], partner).wait_recv()

    def z_sent(view, send, recv):
        for k in range(2 * nz - 1):
            z_copy(view, send, recv, k, tp, partner).wait_send()

    def pick(sems):
        return lambda i: sems.at[i]

    def token_view(slot):
        return x.at[:, at(slot * cl, cl)]

    own_tokens().wait()
    gather_wait(token_place, token_sems)
    z_send(token_view, pick(zs), pick(zr))
    for k in range(1, n):
        route_copy(k, origin[k]).wait_recv()
    for f in range(n):
        routes[f * rows : (f + 1) * rows, : 2 * topk] = rland[f].T
    z_relay(token_view, pick(zs), pick(zr))
    z_finish(token_view, pick(zs), pick(zr))

    block = min(512, total_rows)

    def norms(i, carry):
        part_rows = at(i * 128, 128)
        sums = jnp.zeros((128, 1), jnp.float32)
        for c in range(0, d, 512):
            v = x[part_rows, c : c + 512].astype(jnp.float32)
            sums = sums + jnp.sum(v * v, axis=1, keepdims=True)
        inv[part_rows, :] = jnp.broadcast_to(lax.rsqrt(sums / d + norm_eps), (128, inv.shape[1]))
        return carry

    lax.fori_loop(0, total_rows // 128, norms, 0)

    def down_place(c, who):
        cb, eg = c // neg, lax.rem(c, neg)
        return dout.at[pl.ds(eg * ge, ge), at(who * hd, hd), at(cb * cw, cw)]

    def down_copy(k, c, source):
        return pltpu.make_async_remote_copy(
            src_ref=dsb.at[k - 1, c],
            dst_ref=down_place(c, source),
            send_sem=dss.at[k - 1, c],
            recv_sem=drs.at[k - 1, c],
            device_id=to_fs(k),
            device_id_type=MESH,
        )

    def produce_down():
        for k in order:
            dload(0, k).start()

        def step(c, carry):
            pending = None
            for k in order:
                dload(c, k).wait()
                for e in range(ge):
                    value = dfb[k, e].astype(jnp.bfloat16)
                    if k == 0:
                        cb, eg = c // neg, lax.rem(c, neg)
                        dout[eg * ge + e, at(me * hd, hd), at(cb * cw, cw)] = value
                    else:
                        dsb[k - 1, c, e] = value

                @pl.when(c + 1 < chunks)
                def _():
                    dload(c + 1, k).start()

                if pending is not None:
                    down_copy(pending, c, me).start()
                pending = k
            return carry

        lax.fori_loop(0, chunks, step, 0)

    def hid_view(i):
        return lambda slot: hid.at[slot, i]

    def hid_sem(sems, i):
        return lambda k: sems.at[i, k]

    def hid_args(i):
        return hid_view(i), hid_sem(hs, i), hid_sem(hr, i)

    def consume(i, carry):
        for w in range(2):
            for k in range(1, n):
                weight_copy(w, k, 0, i, origin[k]).wait_recv()
        w_all = jnp.concatenate(
            [gout[pl.ds(i * group, group)].reshape(gl, d), uout[pl.ds(i * group, group)].reshape(gl, d)], axis=0
        )

        def rows_step(r, c):
            rs = at(r * block, block)
            h = silu_mul(nt_dot(x[rs, :], w_all), inv[rs, :gl])
            lane = lax.broadcasted_iota(jnp.int32, h.shape, 1)
            expert = (me * le + group * i + lane // hl).astype(jnp.float32)
            weight = jnp.zeros(h.shape, jnp.float32)
            for k in range(topk):
                weight = weight + jnp.where(
                    routes[rs, k : k + 1] == expert, routes[rs, topk + k : topk + k + 1], 0.0
                )
            hid[tp, i, rs, :] = (h * weight).astype(jnp.bfloat16)
            return c

        if total_rows == block:
            rows_step(0, 0)
        else:
            lax.fori_loop(0, total_rows // block, rows_step, 0)

        @pl.when(i > 0)
        def _():
            z_relay(*hid_args(i - 1))

        z_send(*hid_args(i))

        if pairs > slots:

            @pl.when(i == pairs - slots - 1)
            def _():
                for q in range(2):
                    gather_relay(small_place(q), small_sems[q])

        @pl.when(i + slots < pairs)
        def _():
            for w in range(2):
                for k in range(1, n):
                    weight_copy(w, k, lax.rem(i, slots), i, me).wait_send()
            produce(i + slots)

        if pairs > slots:

            @pl.when(i == pairs - slots - 1)
            def _():
                produce_down()

        return carry

    if pairs == slots:
        for q in range(2):
            gather_relay(small_place(q), small_sems[q])
        produce_down()
    lax.fori_loop(0, pairs, consume, 0)
    z_relay(*hid_args(pairs - 1))

    for i in range(2):
        gather_wait(small_place(i), small_sems[i])
    shared_all = jnp.concatenate([sgo[...], suo[...]], axis=0)

    def shared_step(r, c):
        rs = at(r * block, block)
        h = silu_mul(nt_dot(x[rs, :], shared_all), inv[rs, :hl])
        wide = jnp.concatenate([h] * group, axis=1)
        lane = lax.broadcasted_iota(jnp.int32, wide.shape, 1)
        hid[tp, pairs, rs, :] = jnp.where(lane // hl == lax.rem(tp, sources), wide, 0.0).astype(jnp.bfloat16)
        return c

    if total_rows == block:
        shared_step(0, 0)
    else:
        lax.fori_loop(0, total_rows // block, shared_step, 0)
    z_send(*hid_args(pairs))

    def finish(i, carry):
        z_finish(*hid_args(i))
        return carry

    lax.fori_loop(0, pairs, finish, 0)
    z_relay(*hid_args(pairs))
    z_finish(*hid_args(pairs))

    def part_copy(k, cb, who):
        return pltpu.make_async_remote_copy(
            src_ref=part.at[cb, at(who * rows, rows)],
            dst_ref=landed.at[cb, k - 1],
            send_sem=cs.at[cb, k - 1],
            recv_sem=cr.at[cb, k - 1],
            device_id=to_fs(k),
            device_id_type=MESH,
        )

    per = ge // group
    mine = at(me * rows, rows)

    def down_step(c, carry):
        cb, eg = c // neg, lax.rem(c, neg)
        for k in range(1, n):
            down_copy(k, c, origin[k]).wait_recv()
        left, right = [], []
        for p in range(per):
            pair = eg * per + p
            for s in range(ntp):
                left.append(hid.at[s, pair])
                right.append(
                    dout[pl.ds(pair * group, group), s * hl : (s + 1) * hl, at(cb * cw, cw)].reshape(gl, cw)
                )
        down = jnp.concatenate(right, axis=0)

        def rows_step(r, q):
            rs = at(r * block, block)
            lhs = jnp.concatenate([ref[rs, :] for ref in left], axis=1)
            total = jnp.dot(lhs, down, preferred_element_type=jnp.float32)

            @pl.when(eg == 0)
            def _():
                units = functools.reduce(jnp.add, [hid[me * sources + q, pairs, rs, :hd] for q in range(sources)])
                shared = jnp.dot(units, ssb[:, at(cb * cw, cw)], preferred_element_type=jnp.float32)
                acc[rs, :] = total + shared

            @pl.when(eg > 0)
            def _():
                acc[rs, :] += total

            return q

        if total_rows == block:
            rows_step(0, 0)
        else:
            lax.fori_loop(0, total_rows // block, rows_step, 0)

        if cols > 1:

            @pl.when((eg == neg - 1) & (cb < cols - 1))
            def _():
                part[cb] = acc[...].astype(jnp.bfloat16)
                own[:, at(cb * cw, cw)] = acc[mine, :]
                for k in range(1, n):
                    part_copy(k, cb, dest[k]).start()

        return carry

    lax.fori_loop(0, chunks, down_step, 0)
    fold = rows // cols
    for k in range(1, n):
        to = mate(me, k, n)
        lasts[k - 1][:hd, :] = ssb[...]
        for c in range(cols):
            lasts[k - 1][hd:, c * cw : (c + 1) * cw] = acc[at(to * rows + c * fold, fold), :].astype(jnp.bfloat16)
    own[:, cl - cw :] = acc[mine, :]

    for k in range(1, n):
        route_copy(k, me).wait_send()
    gather_sent(token_place, token_sems)
    for i in range(2):
        gather_sent(small_place(i), small_sems[i])
    z_sent(token_view, pick(zs), pick(zr))

    def sent(i, carry):
        z_sent(*hid_args(i))
        return carry

    lax.fori_loop(0, pairs + 1, sent, 0)

    def weights_sent(j, carry):
        for w in range(2):
            for k in range(1, n):
                weight_copy(w, k, lax.rem(j, slots), j, me).wait_send()
        return carry

    lax.fori_loop(pairs - slots, pairs, weights_sent, 0)

    def down_sent(c, carry):
        for k in range(1, n):
            down_copy(k, c, me).wait_send()
        return carry

    lax.fori_loop(0, chunks, down_sent, 0)

    for cb in range(cols - 1):
        result = own[:, cb * cw : (cb + 1) * cw]
        for k in range(1, n):
            part_copy(k, cb, dest[k]).wait()
            result = result + landed[cb, k - 1].astype(jnp.float32)
        own[:, cb * cw : (cb + 1) * cw] = result


def moe_call(n, ntp, args):
    ids, aff, gain, tokens, gate, up, down, sg, su, sd = args
    bf16, f32 = jnp.bfloat16, jnp.float32
    experts, hl, dl = gate.shape
    _, hd, cl = down.shape
    rows = tokens.shape[0]
    topk = ids.shape[0]
    le, d, hidden, total = experts // n, dl * n, hd * n, rows * n
    group = min(le, max(1, 128 // hl))
    pairs = le // group
    slots = min(4, pairs)
    cols = 2 if cl % 256 == 0 else 1
    cw, early = cl // cols, max(1, cols - 1)
    ge = group * (2 if pairs % 2 == 0 else 1)
    chunks = cols * (le // ge)
    gl = group * hl
    nz = ntp // 2
    vm, dma = pltpu.VMEM, pltpu.SemaphoreType.DMA
    serve = [((le, hl, d), bf16), ((le, hl, d), bf16), ((le, hidden, cl), bf16), ((hl, d), bf16), ((hl, d), bf16)]
    outs = serve + [((rows, cl), f32)] + [((hd + rows // cols, cl), bf16)] * (n - 1)
    pinned = sum(functools.reduce(lambda a, b: a * b, s) * jnp.dtype(t).itemsize for s, t in outs)
    hbm = pl.BlockSpec(memory_space=pltpu.HBM)
    args = [pltpu.with_memory_space_constraint(a, pltpu.HBM) for a in args]
    results = pl.pallas_call(
        functools.partial(moe_kernel, (n, ntp, group, slots, cols, ge)),
        out_shape=tuple(vm(s, t) for s, t in outs),
        in_specs=[hbm] * len(args),
        out_specs=(pl.BlockSpec(memory_space=vm),) * len(outs),
        scratch_shapes=[
            vm(ids.shape, ids.dtype),
            vm(aff.shape, f32),
            vm(gain.shape, f32),
            vm((2 * topk, rows), f32),
            vm((n, 2 * topk, rows), f32),
            vm((total, 128), f32),
            vm((total, d), bf16),
            vm((total, 128), f32),
            vm((n, group, hl, dl), f32),
            vm((2, n - 1, slots, group, hl, dl), bf16),
            vm((n, ge, hd, cw), f32),
            vm((n - 1, chunks, ge, hd, cw), bf16),
            vm(sg.shape, f32),
            vm(su.shape, f32),
            vm(sd.shape, f32),
            vm(sd.shape, bf16),
            vm((ntp, pairs + 1, total, gl), bf16),
            vm((total, cw), f32),
            vm((early, total, cw), bf16),
            vm((early, n - 1, rows, cw), bf16),
            dma((6,)),
            dma((2, n)),
            dma((2, max(4, n))),
            dma,
            dma((2 * nz - 1,)),
            dma((2 * nz - 1,)),
            dma((2, n - 1, slots)),
            dma((2, n - 1, pairs)),
            dma((n - 1, chunks)),
            dma((n - 1, chunks)),
            dma((2, max(4, n))),
            dma((2, max(4, n))),
            dma((pairs + 1, 2 * nz - 1)),
            dma((pairs + 1, 2 * nz - 1)),
            dma((early, n - 1)),
            dma((early, n - 1)),
            dma((2, n)),
        ],
        compiler_params=pltpu.CompilerParams(
            collective_id=0, has_side_effects=True, vmem_limit_bytes=min(60 * 1024 * 1024, vmem_bytes - pinned)
        ),
        cost_estimate=pl.CostEstimate(flops=6 * total * d * hl * le, bytes_accessed=40 * gate.size, transcendentals=0),
    )(*args)

    cut = min(4, le)

    def write(*refs):
        count = len(serve)
        sem = refs[-1]
        copies = []
        for i in range(count):
            step = refs[i].shape[0] // cut
            for c in range(cut):
                piece = pl.ds(c * step, step)
                copies.append(pltpu.make_async_copy(refs[i].at[piece], refs[count + i].at[piece], sem.at[i, c]))
        for c in copies:
            c.start()
        for c in copies:
            c.wait()

    own, sent = results[len(serve)], results[len(serve) + 1 :]
    moved = [lax.ppermute(sent[k - 1], "fs", mate_pairs(k, n)) for k in range(1, n)]
    written = pl.pallas_call(
        write,
        out_shape=tuple(jax.ShapeDtypeStruct(s, t) for s, t in serve),
        in_specs=[pl.BlockSpec(memory_space=vm)] * len(serve),
        out_specs=(hbm,) * len(serve),
        scratch_shapes=[dma((len(serve), cut))],
        compiler_params=pltpu.CompilerParams(vmem_limit_bytes=1024 * 1024),
        cost_estimate=pl.CostEstimate(flops=0, bytes_accessed=10 * pinned, transcendentals=0),
    )(*results[: len(serve)])
    mixed, shared_down = finish_call(n, hd, own, sent[0], moved)
    return (mixed, *written, shared_down)


def finish_kernel(n, hd, own, *refs):
    pieces = refs[:n]
    mixed_ref, down_ref, sem = refs[n:]
    me = lax.axis_index("fs")
    copies = []
    for k in range(n):
        source = mate_origin(me, k, n)
        place = down_ref.at[pl.ds(pl.multiple_of(source * hd, hd), hd)]
        copies.append(pltpu.make_async_copy(pieces[k].at[pl.ds(0, hd)], place, sem.at[k]))
        copies[-1].start()
    rows, cl = own.shape
    fold = pieces[0].shape[0] - hd
    cols = rows // fold
    cw = cl // cols
    early = cl - cw
    if early:
        mixed_ref[:, :early] = own[:, :early].astype(mixed_ref.dtype)
    for c in range(cols):
        part = slice(c * fold, (c + 1) * fold)
        total = own[part, early:]
        for k in range(1, n):
            total = total + pieces[k][hd:, c * cw : (c + 1) * cw].astype(jnp.float32)
        mixed_ref[part, early:] = total.astype(mixed_ref.dtype)
    for c in copies:
        c.wait()


def finish_call(n, hd, own, sent, moved):
    vmem = pl.BlockSpec(memory_space=pltpu.VMEM)
    return pl.pallas_call(
        functools.partial(finish_kernel, n, hd),
        out_shape=(
            jax.ShapeDtypeStruct(own.shape, jnp.bfloat16),
            jax.ShapeDtypeStruct((n * hd, own.shape[1]), jnp.bfloat16),
        ),
        in_specs=[vmem] * (n + 1),
        out_specs=(vmem, pl.BlockSpec(memory_space=pltpu.HBM)),
        scratch_shapes=[pltpu.SemaphoreType.DMA((n,))],
        compiler_params=pltpu.CompilerParams(vmem_limit_bytes=4 * 1024 * 1024),
    )(own, sent, *moved)


def body(
    n,
    ntp,
    tokens,
    expert_ids,
    affinity,
    norm_gain,
    gate_train,
    up_train,
    down_train,
    shared_gate_train,
    shared_up_train,
    shared_down_train,
):
    return moe_call(
        n,
        ntp,
        [
            expert_ids.T,
            affinity.T,
            norm_gain[None, :],
            tokens,
            gate_train,
            up_train,
            down_train,
            shared_gate_train,
            shared_up_train,
            shared_down_train,
        ],
    )


def solution(mesh):
    return jax.shard_map(
        functools.partial(body, mesh.shape["fs"], mesh.shape["tp"]),
        mesh=mesh,
        in_specs=(
            P("fs", "tp"),
            P("fs", None),
            P("fs", None),
            P("fs"),
            P(None, "tp", "fs"),
            P(None, "tp", "fs"),
            P(None, "fs", "tp"),
            P("tp", "fs"),
            P("tp", "fs"),
            P("fs", "tp"),
        ),
        out_specs=(
            P("fs", "tp"),
            P("fs", "tp", None),
            P("fs", "tp", None),
            P("fs", None, "tp"),
            P("tp", None),
            P("tp", None),
            P(None, "tp"),
        ),
        check_vma=False,
    )
```

```python
import functools

import jax
import jax.numpy as jnp
from jax import lax
from jax.experimental import pallas as pl
from jax.experimental.pallas import tpu as pltpu
from jax.sharding import PartitionSpec as P

MESH = pl.DeviceIdType.MESH

norm_eps = 1e-06
routed_scale = 2.5
vmem_bytes = 66900000


def nt_dot(a, b):
    return lax.dot_general(a, b, (((1,), (1,)), ((), ())), preferred_element_type=jnp.float32)


def mate(me, k, n):
    if n & (n - 1):
        return lax.rem(me + k, n)
    other, bit = 0, 1
    while bit < n:
        other = other + bit * lax.rem(lax.div(me, bit) + k // bit, 2)
        bit *= 2
    return other


def mate_origin(me, k, n):
    return lax.rem(me + n - k, n) if n & (n - 1) else mate(me, k, n)


def mate_pairs(k, n):
    return [(i, (i + k) % n if n & (n - 1) else i ^ k) for i in range(n)]


def silu_mul(acc, scale):
    half = acc.shape[1] // 2
    gate = acc[:, :half] * scale
    up = acc[:, half:] * scale
    return gate / (1.0 + jnp.exp(-gate)) * up


def moe_kernel(cfg, *refs):
    n, ntp, group, slots, cols, ge = cfg
    (ids_ref, aff_ref, gain_ref, tok_ref, gate_ref, up_ref, down_ref, sg_ref, su_ref, sd_ref) = refs[:10]
    (gout, uout, dout, sgo, suo, own) = refs[10:16]
    lasts = refs[16 : 15 + n]
    refs = refs[15 + n :]
    (idv, affv, gainv, rbuf, rland, routes, x, inv, fbuf, sbuf, dfb, dsb) = refs[:12]
    (gfb, ufb, sfb, ssb, hid, acc, part, landed) = refs[12:20]
    (isem, lsem, tsem, osem, zs, zr, gss, grs, dss, drs, mss, mrs, hs, hr, cs, cr, rsem) = refs[20:]

    me = lax.axis_index("fs")
    tp = lax.axis_index("tp")
    dest = [lax.rem(me + k, n) for k in range(n)]
    origin = [lax.rem(me + n - k, n) for k in range(n)]
    nz = ntp // 2
    partner = tp + 1 - 2 * lax.rem(tp, 2)
    zdest = [lax.rem(tp + 2 * k, ntp) for k in range(nz)]
    zorigin = [lax.rem(tp + ntp - 2 * k, ntp) for k in range(nz)]
    porigin = [lax.rem(partner + ntp - 2 * k, ntp) for k in range(nz)]

    rows = tok_ref.shape[0]
    total_rows = n * rows
    topk = ids_ref.shape[0]
    le, hl, d = gout.shape
    dl = d // n
    hd = down_ref.shape[1]
    sources = hd // hl
    cl = down_ref.shape[2]
    pairs = le // group
    gl = group * hl
    cw = cl // cols
    neg = le // ge
    chunks = cols * neg
    order = list(range(n - 1, -1, -1))

    def at(first, size):
        return pl.ds(pl.multiple_of(first, size), size)

    def to_fs(k):
        return {"fs": dest[k]}

    smalls = [(gfb, sgo), (ufb, suo)]
    early = [(ids_ref, idv), (aff_ref, affv), (gain_ref, gainv), (sg_ref, gfb), (su_ref, ufb), (sd_ref, sfb)]

    def early_load(i):
        return pltpu.make_async_copy(early[i][0], early[i][1], isem.at[i])

    weights = [gate_ref, up_ref]
    wouts = [gout, uout]

    def load(w, j, k):
        return pltpu.make_async_copy(
            weights[w].at[pl.ds(dest[k] * le + j * group, group)], fbuf.at[k], lsem.at[0, k]
        )

    def dload(c, k):
        cb, eg = c // neg, lax.rem(c, neg)
        return pltpu.make_async_copy(
            down_ref.at[pl.ds(dest[k] * le + eg * ge, ge), :, at(cb * cw, cw)], dfb.at[k], lsem.at[1, k]
        )

    def own_tokens():
        return pltpu.make_async_copy(tok_ref, x.at[at(me * rows, rows), at(tp * cl, cl)], osem)

    barrier = pltpu.get_barrier_semaphore()
    for k in range(1, n):
        pl.semaphore_signal(barrier, inc=1, device_id=to_fs(k), device_id_type=MESH)
    for k in range(1, nz):
        pl.semaphore_signal(barrier, inc=1, device_id={"tp": zdest[k]}, device_id_type=MESH)
    pl.semaphore_signal(barrier, inc=1, device_id={"tp": partner}, device_id_type=MESH)
    for i in range(len(early)):
        early_load(i).start()
    for k in order:
        load(0, 0, k).start()
    own_tokens().start()

    for i in range(3):
        early_load(i).wait()
    affinity = affv[...]
    route = jnp.concatenate(
        [idv[...].astype(jnp.float32), routed_scale * affinity / jnp.sum(affinity, axis=0, keepdims=True)], axis=0
    )
    rbuf[...] = route
    rland[me] = route
    own_tokens().wait()
    pl.semaphore_wait(barrier, n - 1 + nz)

    relay = n == 4
    near = [mate(me, k, n) for k in (1, 2)] if relay else []
    far = mate(me, 3, n) if relay else None

    def fs_copy(src, dst, sems, index, to):
        return pltpu.make_async_remote_copy(
            src_ref=src,
            dst_ref=dst,
            send_sem=sems[0](index),
            recv_sem=sems[1](index),
            device_id={"fs": to},
            device_id_type=MESH,
        )

    def gather_start(src, view, sems):
        for i, to in enumerate(near if relay else dest[1:]):
            fs_copy(src, view(me, None), sems, i, to).start()

    def gather_relay(view, sems):
        if relay:
            for i in range(2):
                whole = view(near[i], None)
                fs_copy(whole, whole, sems, i, near[i]).wait_recv()
                half = view(near[i], i)
                fs_copy(half, half, sems, 2 + i, near[1 - i]).start()

    def gather_wait(view, sems):
        if relay:
            for i in range(2):
                half = view(far, i)
                fs_copy(half, half, sems, 2 + i, near[1 - i]).wait_recv()
        else:
            for k in range(1, n):
                whole = view(origin[k], None)
                fs_copy(whole, whole, sems, k - 1, dest[k]).wait_recv()

    def gather_sent(view, sems):
        for i in range(2 if relay else n - 1):
            whole = view(me, None)
            fs_copy(whole, whole, sems, i, dest[1]).wait_send()
        if relay:
            for i in range(2):
                half = view(near[i], i)
                fs_copy(half, half, sems, 2 + i, near[1 - i]).wait_send()

    def token_place(who, half):
        size = rows if half is None else rows // 2
        return x.at[at(who * rows + (half or 0) * size, size), at(tp * cl, cl)]

    token_sems = (lambda i: tsem.at[0, i], lambda i: tsem.at[1, i])

    def route_copy(k, source):
        return pltpu.make_async_remote_copy(
            src_ref=rbuf,
            dst_ref=rland.at[source],
            send_sem=rsem.at[0, k],
            recv_sem=rsem.at[1, k],
            device_id=to_fs(k),
            device_id_type=MESH,
        )

    gather_start(token_place(me, None), token_place, token_sems)

    def weight_copy(w, k, slot, j, source):
        return pltpu.make_async_remote_copy(
            src_ref=sbuf.at[w, k - 1, slot],
            dst_ref=wouts[w].at[pl.ds(j * group, group), :, at(source * dl, dl)],
            send_sem=gss.at[w, k - 1, slot],
            recv_sem=grs.at[w, k - 1, j],
            device_id=to_fs(k),
            device_id_type=MESH,
        )

    def produce(j):
        slot = lax.rem(j, slots)
        for w in range(2):
            pending = None
            for k in order:
                load(w, j, k).wait()
                for c in range(group):
                    value = (fbuf[k, c] * gainv[...]).astype(jnp.bfloat16)
                    if k == 0:
                        wouts[w][j * group + c, :, at(me * dl, dl)] = value
                    else:
                        sbuf[w, k - 1, slot, c] = value
                if w == 0:
                    load(1, j, k).start()
                else:

                    @pl.when(j + 1 < pairs)
                    def _():
                        load(0, j + 1, k).start()

                if pending is not None:
                    weight_copy(w, pending, slot, j, me).start()
                pending = k

    def first(j, carry):
        produce(j)

        @pl.when(j == 0)
        def _():
            gather_relay(token_place, token_sems)

        return carry

    lax.fori_loop(0, slots, first, 0)

    for k in range(1, n):
        route_copy(k, me).start()

    def small_place(i):
        def view(who, half):
            size = hl if half is None else hl // 2
            return smalls[i][1].at[pl.ds((half or 0) * size, size), at(who * dl, dl)]

        return view

    small_sems = [(lambda k, i=i: mss.at[i, k], lambda k, i=i: mrs.at[i, k]) for i in range(2)]
    for i in range(2):
        early_load(3 + i).wait()
        smalls[i][1][:, at(me * dl, dl)] = (smalls[i][0][...] * gainv[...]).astype(jnp.bfloat16)
    for i in range(2):
        gather_start(small_place(i)(me, None), small_place(i), small_sems[i])
    early_load(5).wait()
    ssb[...] = sfb[...].astype(jnp.bfloat16)

    def z_copy(view, send, recv, index, slot, to):
        return pltpu.make_async_remote_copy(
            src_ref=view(slot),
            dst_ref=view(slot),
            send_sem=send(index),
            recv_sem=recv(index),
            device_id={"tp": to},
            device_id_type=MESH,
        )

    def z_send(view, send, recv):
        for k in range(1, nz):
            z_copy(view, send, recv, k, tp, zdest[k]).start()
        z_copy(view, send, recv, 0, tp, partner).start()

    def z_relay(view, send, recv):
        for k in range(1, nz):
            z_copy(view, send, recv, k, zorigin[k], zdest[k]).wait_recv()
            z_copy(view, send, recv, nz - 1 + k, zorigin[k], partner).start()

    def z_finish(view, send, recv):
        z_copy(view, send, recv, 0, partner, partner).wait_recv()
        for k in range(1, nz):
            z_copy(view, send, recv, nz - 1 + k, porigin[k], partner).wait_recv()

    def z_sent(view, send, recv):
        for k in range(2 * nz - 1):
            z_copy(view, send, recv, k, tp, partner).wait_send()

    def pick(sems):
        return lambda i: sems.at[i]

    def token_view(slot):
        return x.at[:, at(slot * cl, cl)]

    gather_wait(token_place, token_sems)
    z_send(token_view, pick(zs), pick(zr))
    for k in range(1, n):
        route_copy(k, origin[k]).wait_recv()
    for f in range(n):
        routes[f * rows : (f + 1) * rows, : 2 * topk] = rland[f].T
    z_relay(token_view, pick(zs), pick(zr))
    z_finish(token_view, pick(zs), pick(zr))

    block = min(512, total_rows)

    def norms(i, carry):
        part_rows = at(i * 128, 128)
        sums = jnp.zeros((128, 1), jnp.float32)
        for c in range(0, d, 512):
            v = x[part_rows, c : c + 512].astype(jnp.float32)
            sums = sums + jnp.sum(v * v, axis=1, keepdims=True)
        inv[part_rows, :] = jnp.broadcast_to(lax.rsqrt(sums / d + norm_eps), (128, inv.shape[1]))
        return carry

    lax.fori_loop(0, total_rows // 128, norms, 0)

    def down_place(c, who):
        cb, eg = c // neg, lax.rem(c, neg)
        return dout.at[pl.ds(eg * ge, ge), at(who * hd, hd), at(cb * cw, cw)]

    def down_copy(k, c, source):
        return pltpu.make_async_remote_copy(
            src_ref=dsb.at[k - 1, c],
            dst_ref=down_place(c, source),
            send_sem=dss.at[k - 1, c],
            recv_sem=drs.at[k - 1, c],
            device_id=to_fs(k),
            device_id_type=MESH,
        )

    def produce_down():
        for k in order:
            dload(0, k).start()

        def step(c, carry):
            pending = None
            for k in order:
                dload(c, k).wait()
                for e in range(ge):
                    value = dfb[k, e].astype(jnp.bfloat16)
                    if k == 0:
                        cb, eg = c // neg, lax.rem(c, neg)
                        dout[eg * ge + e, at(me * hd, hd), at(cb * cw, cw)] = value
                    else:
                        dsb[k - 1, c, e] = value

                @pl.when(c + 1 < chunks)
                def _():
                    dload(c + 1, k).start()

                if pending is not None:
                    down_copy(pending, c, me).start()
                pending = k
            return carry

        lax.fori_loop(0, chunks, step, 0)

    def hid_view(i):
        return lambda slot: hid.at[slot, i]

    def hid_sem(sems, i):
        return lambda k: sems.at[i, k]

    def hid_args(i):
        return hid_view(i), hid_sem(hs, i), hid_sem(hr, i)

    def consume(i, carry):
        for w in range(2):
            for k in range(1, n):
                weight_copy(w, k, 0, i, origin[k]).wait_recv()
        w_all = jnp.concatenate(
            [gout[pl.ds(i * group, group)].reshape(gl, d), uout[pl.ds(i * group, group)].reshape(gl, d)], axis=0
        )

        def rows_step(r, c):
            rs = at(r * block, block)
            h = silu_mul(nt_dot(x[rs, :], w_all), inv[rs, :gl])
            lane = lax.broadcasted_iota(jnp.int32, h.shape, 1)
            expert = (me * le + group * i + lane // hl).astype(jnp.float32)
            weight = jnp.zeros(h.shape, jnp.float32)
            for k in range(topk):
                weight = weight + jnp.where(
                    routes[rs, k : k + 1] == expert, routes[rs, topk + k : topk + k + 1], 0.0
                )
            hid[tp, i, rs, :] = (h * weight).astype(jnp.bfloat16)
            return c

        if total_rows == block:
            rows_step(0, 0)
        else:
            lax.fori_loop(0, total_rows // block, rows_step, 0)

        @pl.when(i > 0)
        def _():
            z_relay(*hid_args(i - 1))

        z_send(*hid_args(i))

        if pairs > slots:

            @pl.when(i == pairs - slots - 1)
            def _():
                for q in range(2):
                    gather_relay(small_place(q), small_sems[q])

        @pl.when(i + slots < pairs)
        def _():
            for w in range(2):
                for k in range(1, n):
                    weight_copy(w, k, lax.rem(i, slots), i, me).wait_send()
            produce(i + slots)

        if pairs > slots:

            @pl.when(i == pairs - slots - 1)
            def _():
                produce_down()

        return carry

    if pairs == slots:
        for q in range(2):
            gather_relay(small_place(q), small_sems[q])
        produce_down()
    lax.fori_loop(0, pairs, consume, 0)
    z_relay(*hid_args(pairs - 1))

    for i in range(2):
        gather_wait(small_place(i), small_sems[i])
    shared_all = jnp.concatenate([sgo[...], suo[...]], axis=0)

    def shared_step(r, c):
        rs = at(r * block, block)
        h = silu_mul(nt_dot(x[rs, :], shared_all), inv[rs, :hl])
        wide = jnp.concatenate([h] * group, axis=1)
        lane = lax.broadcasted_iota(jnp.int32, wide.shape, 1)
        hid[tp, pairs, rs, :] = jnp.where(lane // hl == lax.rem(tp, sources), wide, 0.0).astype(jnp.bfloat16)
        return c

    if total_rows == block:
        shared_step(0, 0)
    else:
        lax.fori_loop(0, total_rows // block, shared_step, 0)
    z_send(*hid_args(pairs))

    def finish(i, carry):
        z_finish(*hid_args(i))
        return carry

    lax.fori_loop(0, pairs, finish, 0)
    z_relay(*hid_args(pairs))
    z_finish(*hid_args(pairs))

    def part_copy(k, cb, who):
        return pltpu.make_async_remote_copy(
            src_ref=part.at[cb, at(who * rows, rows)],
            dst_ref=landed.at[cb, k - 1],
            send_sem=cs.at[cb, k - 1],
            recv_sem=cr.at[cb, k - 1],
            device_id=to_fs(k),
            device_id_type=MESH,
        )

    per = ge // group
    mine = at(me * rows, rows)

    def down_step(c, carry):
        cb, eg = c // neg, lax.rem(c, neg)
        for k in range(1, n):
            down_copy(k, c, origin[k]).wait_recv()
        left, right = [], []
        for p in range(per):
            pair = eg * per + p
            for s in range(ntp):
                left.append(hid.at[s, pair])
                right.append(
                    dout[pl.ds(pair * group, group), s * hl : (s + 1) * hl, at(cb * cw, cw)].reshape(gl, cw)
                )
        down = jnp.concatenate(right, axis=0)

        def rows_step(r, q):
            rs = at(r * block, block)
            lhs = jnp.concatenate([ref[rs, :] for ref in left], axis=1)
            total = jnp.dot(lhs, down, preferred_element_type=jnp.float32)

            @pl.when(eg == 0)
            def _():
                units = functools.reduce(jnp.add, [hid[me * sources + q, pairs, rs, :hd] for q in range(sources)])
                shared = jnp.dot(units, ssb[:, at(cb * cw, cw)], preferred_element_type=jnp.float32)
                acc[rs, :] = total + shared

            @pl.when(eg > 0)
            def _():
                acc[rs, :] += total

            return q

        if total_rows == block:
            rows_step(0, 0)
        else:
            lax.fori_loop(0, total_rows // block, rows_step, 0)

        if cols > 1:

            @pl.when((eg == neg - 1) & (cb < cols - 1))
            def _():
                part[cb] = acc[...].astype(jnp.bfloat16)
                own[:, at(cb * cw, cw)] = acc[mine, :]
                for k in range(1, n):
                    part_copy(k, cb, dest[k]).start()

        return carry

    lax.fori_loop(0, chunks, down_step, 0)
    fold = rows // cols
    for k in range(1, n):
        to = mate(me, k, n)
        lasts[k - 1][:hd, :] = ssb[...]
        for c in range(cols):
            lasts[k - 1][hd:, c * cw : (c + 1) * cw] = acc[at(to * rows + c * fold, fold), :].astype(jnp.bfloat16)
    own[:, cl - cw :] = acc[mine, :]

    for k in range(1, n):
        route_copy(k, me).wait_send()
    gather_sent(token_place, token_sems)
    for i in range(2):
        gather_sent(small_place(i), small_sems[i])
    z_sent(token_view, pick(zs), pick(zr))

    def sent(i, carry):
        z_sent(*hid_args(i))
        return carry

    lax.fori_loop(0, pairs + 1, sent, 0)

    def weights_sent(j, carry):
        for w in range(2):
            for k in range(1, n):
                weight_copy(w, k, lax.rem(j, slots), j, me).wait_send()
        return carry

    lax.fori_loop(pairs - slots, pairs, weights_sent, 0)

    def down_sent(c, carry):
        for k in range(1, n):
            down_copy(k, c, me).wait_send()
        return carry

    lax.fori_loop(0, chunks, down_sent, 0)

    for cb in range(cols - 1):
        result = own[:, cb * cw : (cb + 1) * cw]
        for k in range(1, n):
            part_copy(k, cb, dest[k]).wait()
            result = result + landed[cb, k - 1].astype(jnp.float32)
        own[:, cb * cw : (cb + 1) * cw] = result


def moe_call(n, ntp, args):
    ids, aff, gain, tokens, gate, up, down, sg, su, sd = args
    bf16, f32 = jnp.bfloat16, jnp.float32
    experts, hl, dl = gate.shape
    _, hd, cl = down.shape
    rows = tokens.shape[0]
    topk = ids.shape[0]
    le, d, hidden, total = experts // n, dl * n, hd * n, rows * n
    group = min(le, max(1, 128 // hl))
    pairs = le // group
    slots = min(6, pairs)
    cols = 2 if cl % 256 == 0 else 1
    cw, early = cl // cols, max(1, cols - 1)
    ge = group * (2 if pairs % 2 == 0 else 1)
    chunks = cols * (le // ge)
    gl = group * hl
    nz = ntp // 2
    vm, dma = pltpu.VMEM, pltpu.SemaphoreType.DMA
    serve = [((le, hl, d), bf16), ((le, hl, d), bf16), ((le, hidden, cl), bf16), ((hl, d), bf16), ((hl, d), bf16)]
    outs = serve + [((rows, cl), f32)] + [((hd + rows // cols, cl), bf16)] * (n - 1)
    pinned = sum(functools.reduce(lambda a, b: a * b, s) * jnp.dtype(t).itemsize for s, t in outs)
    hbm = pl.BlockSpec(memory_space=pltpu.HBM)
    args = [pltpu.with_memory_space_constraint(a, pltpu.HBM) for a in args]
    results = pl.pallas_call(
        functools.partial(moe_kernel, (n, ntp, group, slots, cols, ge)),
        out_shape=tuple(vm(s, t) for s, t in outs),
        in_specs=[hbm] * len(args),
        out_specs=(pl.BlockSpec(memory_space=vm),) * len(outs),
        scratch_shapes=[
            vm(ids.shape, ids.dtype),
            vm(aff.shape, f32),
            vm(gain.shape, f32),
            vm((2 * topk, rows), f32),
            vm((n, 2 * topk, rows), f32),
            vm((total, 128), f32),
            vm((total, d), bf16),
            vm((total, 128), f32),
            vm((n, group, hl, dl), f32),
            vm((2, n - 1, slots, group, hl, dl), bf16),
            vm((n, ge, hd, cw), f32),
            vm((n - 1, chunks, ge, hd, cw), bf16),
            vm(sg.shape, f32),
            vm(su.shape, f32),
            vm(sd.shape, f32),
            vm(sd.shape, bf16),
            vm((ntp, pairs + 1, total, gl), bf16),
            vm((total, cw), f32),
            vm((early, total, cw), bf16),
            vm((early, n - 1, rows, cw), bf16),
            dma((6,)),
            dma((2, n)),
            dma((2, max(4, n))),
            dma,
            dma((2 * nz - 1,)),
            dma((2 * nz - 1,)),
            dma((2, n - 1, slots)),
            dma((2, n - 1, pairs)),
            dma((n - 1, chunks)),
            dma((n - 1, chunks)),
            dma((2, max(4, n))),
            dma((2, max(4, n))),
            dma((pairs + 1, 2 * nz - 1)),
            dma((pairs + 1, 2 * nz - 1)),
            dma((early, n - 1)),
            dma((early, n - 1)),
            dma((2, n)),
        ],
        compiler_params=pltpu.CompilerParams(
            collective_id=0, has_side_effects=True, vmem_limit_bytes=min(60 * 1024 * 1024, vmem_bytes - pinned)
        ),
        cost_estimate=pl.CostEstimate(flops=6 * total * d * hl * le, bytes_accessed=40 * gate.size, transcendentals=0),
    )(*args)

    cut = min(4, le)

    def write(*refs):
        count = len(serve)
        sem = refs[-1]
        copies = []
        for i in range(count):
            step = refs[i].shape[0] // cut
            for c in range(cut):
                piece = pl.ds(c * step, step)
                copies.append(pltpu.make_async_copy(refs[i].at[piece], refs[count + i].at[piece], sem.at[i, c]))
        for c in copies:
            c.start()
        for c in copies:
            c.wait()

    own, sent = results[len(serve)], results[len(serve) + 1 :]
    moved = [lax.ppermute(sent[k - 1], "fs", mate_pairs(k, n)) for k in range(1, n)]
    written = pl.pallas_call(
        write,
        out_shape=tuple(jax.ShapeDtypeStruct(s, t) for s, t in serve),
        in_specs=[pl.BlockSpec(memory_space=vm)] * len(serve),
        out_specs=(hbm,) * len(serve),
        scratch_shapes=[dma((len(serve), cut))],
        compiler_params=pltpu.CompilerParams(vmem_limit_bytes=1024 * 1024),
        cost_estimate=pl.CostEstimate(flops=0, bytes_accessed=10 * pinned, transcendentals=0),
    )(*results[: len(serve)])
    mixed, shared_down = finish_call(n, hd, own, sent[0], moved)
    return (mixed, *written, shared_down)


def finish_kernel(n, hd, own, *refs):
    pieces = refs[:n]
    mixed_ref, down_ref, sem = refs[n:]
    me = lax.axis_index("fs")
    copies = []
    for k in range(n):
        source = mate_origin(me, k, n)
        place = down_ref.at[pl.ds(pl.multiple_of(source * hd, hd), hd)]
        copies.append(pltpu.make_async_copy(pieces[k].at[pl.ds(0, hd)], place, sem.at[k]))
        copies[-1].start()
    rows, cl = own.shape
    fold = pieces[0].shape[0] - hd
    cols = rows // fold
    cw = cl // cols
    early = cl - cw
    if early:
        mixed_ref[:, :early] = own[:, :early].astype(mixed_ref.dtype)
    for c in range(cols):
        part = slice(c * fold, (c + 1) * fold)
        total = own[part, early:]
        for k in range(1, n):
            total = total + pieces[k][hd:, c * cw : (c + 1) * cw].astype(jnp.float32)
        mixed_ref[part, early:] = total.astype(mixed_ref.dtype)
    for c in copies:
        c.wait()


def finish_call(n, hd, own, sent, moved):
    vmem = pl.BlockSpec(memory_space=pltpu.VMEM)
    return pl.pallas_call(
        functools.partial(finish_kernel, n, hd),
        out_shape=(
            jax.ShapeDtypeStruct(own.shape, jnp.bfloat16),
            jax.ShapeDtypeStruct((n * hd, own.shape[1]), jnp.bfloat16),
        ),
        in_specs=[vmem] * (n + 1),
        out_specs=(vmem, pl.BlockSpec(memory_space=pltpu.HBM)),
        scratch_shapes=[pltpu.SemaphoreType.DMA((n,))],
        compiler_params=pltpu.CompilerParams(vmem_limit_bytes=4 * 1024 * 1024),
    )(own, sent, *moved)


def body(
    n,
    ntp,
    tokens,
    expert_ids,
    affinity,
    norm_gain,
    gate_train,
    up_train,
    down_train,
    shared_gate_train,
    shared_up_train,
    shared_down_train,
):
    return moe_call(
        n,
        ntp,
        [
            expert_ids.T,
            affinity.T,
            norm_gain[None, :],
            tokens,
            gate_train,
            up_train,
            down_train,
            shared_gate_train,
            shared_up_train,
            shared_down_train,
        ],
    )


def solution(mesh):
    return jax.shard_map(
        functools.partial(body, mesh.shape["fs"], mesh.shape["tp"]),
        mesh=mesh,
        in_specs=(
            P("fs", "tp"),
            P("fs", None),
            P("fs", None),
            P("fs"),
            P(None, "tp", "fs"),
            P(None, "tp", "fs"),
            P(None, "fs", "tp"),
            P("tp", "fs"),
            P("tp", "fs"),
            P("fs", "tp"),
        ),
        out_specs=(
            P("fs", "tp"),
            P("fs", "tp", None),
            P("fs", "tp", None),
            P("fs", None, "tp"),
            P("tp", None),
            P("tp", None),
            P(None, "tp"),
        ),
        check_vma=False,
    )
```

```python
import functools

import jax
import jax.numpy as jnp
from jax import lax
from jax.experimental import pallas as pl
from jax.experimental.pallas import tpu as pltpu
from jax.sharding import PartitionSpec as P

MESH = pl.DeviceIdType.MESH

norm_eps = 1e-06
routed_scale = 2.5
vmem_bytes = 66900000


def nt_dot(a, b):
    return lax.dot_general(a, b, (((1,), (1,)), ((), ())), preferred_element_type=jnp.float32)


def mate(me, k, n):
    if n & (n - 1):
        return lax.rem(me + k, n)
    other, bit = 0, 1
    while bit < n:
        other = other + bit * lax.rem(lax.div(me, bit) + k // bit, 2)
        bit *= 2
    return other


def mate_origin(me, k, n):
    return lax.rem(me + n - k, n) if n & (n - 1) else mate(me, k, n)


def turn(k, n):
    return k if n & (n - 1) else k ^ (k >> 1)


def mate_pairs(k, n):
    return [(i, (i + k) % n if n & (n - 1) else i ^ k) for i in range(n)]


def silu_mul(acc, scale):
    half = acc.shape[1] // 2
    gate = acc[:, :half] * scale
    up = acc[:, half:] * scale
    return gate / (1.0 + jnp.exp(-gate)) * up


def moe_kernel(cfg, *refs):
    n, ntp, group, slots, cols, ge = cfg
    (ids_ref, aff_ref, gain_ref, tok_ref, gate_ref, up_ref, down_ref, sg_ref, su_ref, sd_ref) = refs[:10]
    (gout, uout, dout, sgo, suo, own) = refs[10:16]
    lasts = refs[16 : 15 + n]
    refs = refs[15 + n :]
    (idv, affv, gainv, rbuf, rland, routes, x, inv, fbuf, sbuf, dfb, dsb) = refs[:12]
    (gfb, ufb, sfb, ssb, hid, acc, part, landed) = refs[12:20]
    (isem, lsem, tsem, osem, zs, zr, gss, grs, dss, drs, mss, mrs, hs, hr, cs, cr, rsem) = refs[20:]

    me = lax.axis_index("fs")
    tp = lax.axis_index("tp")
    dest = [lax.rem(me + k, n) for k in range(n)]
    origin = [lax.rem(me + n - k, n) for k in range(n)]
    nz = ntp // 2
    partner = tp + 1 - 2 * lax.rem(tp, 2)
    zdest = [lax.rem(tp + 2 * k, ntp) for k in range(nz)]
    zorigin = [lax.rem(tp + ntp - 2 * k, ntp) for k in range(nz)]
    porigin = [lax.rem(partner + ntp - 2 * k, ntp) for k in range(nz)]

    rows = tok_ref.shape[0]
    total_rows = n * rows
    topk = ids_ref.shape[0]
    le, hl, d = gout.shape
    dl = d // n
    hd = down_ref.shape[1]
    sources = hd // hl
    cl = down_ref.shape[2]
    pairs = le // group
    gl = group * hl
    cw = cl // cols
    neg = le // ge
    chunks = cols * neg
    order = list(range(n - 1, -1, -1))

    def at(first, size):
        return pl.ds(pl.multiple_of(first, size), size)

    def to_fs(k):
        return {"fs": dest[k]}

    smalls = [(gfb, sgo), (ufb, suo)]
    early = [(ids_ref, idv), (aff_ref, affv), (gain_ref, gainv), (sg_ref, gfb), (su_ref, ufb), (sd_ref, sfb)]

    def early_load(i):
        return pltpu.make_async_copy(early[i][0], early[i][1], isem.at[i])

    weights = [gate_ref, up_ref]
    wouts = [gout, uout]

    def load(w, j, k):
        return pltpu.make_async_copy(
            weights[w].at[pl.ds(dest[k] * le + j * group, group)], fbuf.at[k], lsem.at[0, k]
        )

    def dload(c, k):
        cb, eg = c // neg, lax.rem(c, neg)
        return pltpu.make_async_copy(
            down_ref.at[pl.ds(dest[k] * le + eg * ge, ge), :, at(cb * cw, cw)], dfb.at[k], lsem.at[1, k]
        )

    def own_tokens():
        return pltpu.make_async_copy(tok_ref, x.at[at(me * rows, rows), at(tp * cl, cl)], osem)

    barrier = pltpu.get_barrier_semaphore()
    for k in range(1, n):
        pl.semaphore_signal(barrier, inc=1, device_id=to_fs(k), device_id_type=MESH)
    for k in range(1, nz):
        pl.semaphore_signal(barrier, inc=1, device_id={"tp": zdest[k]}, device_id_type=MESH)
    pl.semaphore_signal(barrier, inc=1, device_id={"tp": partner}, device_id_type=MESH)
    for i in range(len(early)):
        early_load(i).start()
    for k in order:
        load(0, 0, k).start()
    own_tokens().start()

    for i in range(3):
        early_load(i).wait()
    affinity = affv[...]
    route = jnp.concatenate(
        [idv[...].astype(jnp.float32), routed_scale * affinity / jnp.sum(affinity, axis=0, keepdims=True)], axis=0
    )
    rbuf[...] = route
    rland[me] = route
    own_tokens().wait()
    pl.semaphore_wait(barrier, n - 1 + nz)

    relay = n == 4
    near = [mate(me, k, n) for k in (1, 2)] if relay else []
    far = mate(me, 3, n) if relay else None

    def fs_copy(src, dst, sems, index, to):
        return pltpu.make_async_remote_copy(
            src_ref=src,
            dst_ref=dst,
            send_sem=sems[0](index),
            recv_sem=sems[1](index),
            device_id={"fs": to},
            device_id_type=MESH,
        )

    def gather_start(src, view, sems):
        for i, to in enumerate(near if relay else dest[1:]):
            fs_copy(src, view(me, None), sems, i, to).start()

    def gather_relay(view, sems):
        if relay:
            for i in range(2):
                whole = view(near[i], None)
                fs_copy(whole, whole, sems, i, near[i]).wait_recv()
                half = view(near[i], i)
                fs_copy(half, half, sems, 2 + i, near[1 - i]).start()

    def gather_wait(view, sems):
        if relay:
            for i in range(2):
                half = view(far, i)
                fs_copy(half, half, sems, 2 + i, near[1 - i]).wait_recv()
        else:
            for k in range(1, n):
                whole = view(origin[k], None)
                fs_copy(whole, whole, sems, k - 1, dest[k]).wait_recv()

    def gather_sent(view, sems):
        for i in range(2 if relay else n - 1):
            whole = view(me, None)
            fs_copy(whole, whole, sems, i, dest[1]).wait_send()
        if relay:
            for i in range(2):
                half = view(near[i], i)
                fs_copy(half, half, sems, 2 + i, near[1 - i]).wait_send()

    def token_place(who, half):
        size = rows if half is None else rows // 2
        return x.at[at(who * rows + (half or 0) * size, size), at(tp * cl, cl)]

    token_sems = (lambda i: tsem.at[0, i], lambda i: tsem.at[1, i])

    def route_copy(k, source):
        return pltpu.make_async_remote_copy(
            src_ref=rbuf,
            dst_ref=rland.at[source],
            send_sem=rsem.at[0, k],
            recv_sem=rsem.at[1, k],
            device_id=to_fs(k),
            device_id_type=MESH,
        )

    gather_start(token_place(me, None), token_place, token_sems)

    def weight_copy(w, k, slot, j, source):
        return pltpu.make_async_remote_copy(
            src_ref=sbuf.at[w, k - 1, slot],
            dst_ref=wouts[w].at[pl.ds(j * group, group), :, at(source * dl, dl)],
            send_sem=gss.at[w, k - 1, slot],
            recv_sem=grs.at[w, k - 1, j],
            device_id=to_fs(k),
            device_id_type=MESH,
        )

    def produce(j):
        slot = lax.rem(j, slots)
        for w in range(2):
            pending = None
            for k in order:
                load(w, j, k).wait()
                for c in range(group):
                    value = (fbuf[k, c] * gainv[...]).astype(jnp.bfloat16)
                    if k == 0:
                        wouts[w][j * group + c, :, at(me * dl, dl)] = value
                    else:
                        sbuf[w, k - 1, slot, c] = value
                if w == 0:
                    load(1, j, k).start()
                else:

                    @pl.when(j + 1 < pairs)
                    def _():
                        load(0, j + 1, k).start()

                if pending is not None:
                    weight_copy(w, pending, slot, j, me).start()
                pending = k

    def first(j, carry):
        produce(j)

        @pl.when(j == 0)
        def _():
            gather_relay(token_place, token_sems)

        return carry

    lax.fori_loop(0, slots, first, 0)

    for k in range(1, n):
        route_copy(k, me).start()

    def small_place(i):
        def view(who, half):
            size = hl if half is None else hl // 2
            return smalls[i][1].at[pl.ds((half or 0) * size, size), at(who * dl, dl)]

        return view

    small_sems = [(lambda k, i=i: mss.at[i, k], lambda k, i=i: mrs.at[i, k]) for i in range(2)]
    for i in range(2):
        early_load(3 + i).wait()
        smalls[i][1][:, at(me * dl, dl)] = (smalls[i][0][...] * gainv[...]).astype(jnp.bfloat16)
    for i in range(2):
        gather_start(small_place(i)(me, None), small_place(i), small_sems[i])
    early_load(5).wait()
    ssb[...] = sfb[...].astype(jnp.bfloat16)

    def z_copy(view, send, recv, index, slot, to):
        return pltpu.make_async_remote_copy(
            src_ref=view(slot),
            dst_ref=view(slot),
            send_sem=send(index),
            recv_sem=recv(index),
            device_id={"tp": to},
            device_id_type=MESH,
        )

    def z_send(view, send, recv):
        for k in range(1, nz):
            z_copy(view, send, recv, k, tp, zdest[k]).start()
        z_copy(view, send, recv, 0, tp, partner).start()

    def z_relay(view, send, recv):
        for k in range(1, nz):
            z_copy(view, send, recv, k, zorigin[k], zdest[k]).wait_recv()
            z_copy(view, send, recv, nz - 1 + k, zorigin[k], partner).start()

    def z_finish(view, send, recv):
        z_copy(view, send, recv, 0, partner, partner).wait_recv()
        for k in range(1, nz):
            z_copy(view, send, recv, nz - 1 + k, porigin[k], partner).wait_recv()

    def z_sent(view, send, recv):
        for k in range(2 * nz - 1):
            z_copy(view, send, recv, k, tp, partner).wait_send()

    def pick(sems):
        return lambda i: sems.at[i]

    def token_view(slot):
        return x.at[:, at(slot * cl, cl)]

    gather_wait(token_place, token_sems)
    z_send(token_view, pick(zs), pick(zr))
    for k in range(1, n):
        route_copy(k, origin[k]).wait_recv()
    for f in range(n):
        routes[f * rows : (f + 1) * rows, : 2 * topk] = rland[f].T
    z_relay(token_view, pick(zs), pick(zr))
    z_finish(token_view, pick(zs), pick(zr))

    block = min(512, total_rows)

    def norms(i, carry):
        part_rows = at(i * 128, 128)
        sums = jnp.zeros((128, 1), jnp.float32)
        for c in range(0, d, 512):
            v = x[part_rows, c : c + 512].astype(jnp.float32)
            sums = sums + jnp.sum(v * v, axis=1, keepdims=True)
        inv[part_rows, :] = jnp.broadcast_to(lax.rsqrt(sums / d + norm_eps), (128, inv.shape[1]))
        return carry

    lax.fori_loop(0, total_rows // 128, norms, 0)

    def down_place(c, who):
        cb, eg = c // neg, lax.rem(c, neg)
        return dout.at[pl.ds(eg * ge, ge), at(who * hd, hd), at(cb * cw, cw)]

    def down_copy(k, c, source):
        return pltpu.make_async_remote_copy(
            src_ref=dsb.at[k - 1, c],
            dst_ref=down_place(c, source),
            send_sem=dss.at[k - 1, c],
            recv_sem=drs.at[k - 1, c],
            device_id=to_fs(k),
            device_id_type=MESH,
        )

    def produce_down():
        for k in order:
            dload(0, k).start()

        def step(c, carry):
            pending = None
            for k in order:
                dload(c, k).wait()
                for e in range(ge):
                    value = dfb[k, e].astype(jnp.bfloat16)
                    if k == 0:
                        cb, eg = c // neg, lax.rem(c, neg)
                        dout[eg * ge + e, at(me * hd, hd), at(cb * cw, cw)] = value
                    else:
                        dsb[k - 1, c, e] = value

                @pl.when(c + 1 < chunks)
                def _():
                    dload(c + 1, k).start()

                if pending is not None:
                    down_copy(pending, c, me).start()
                pending = k
            return carry

        lax.fori_loop(0, chunks, step, 0)

    def hid_view(i):
        return lambda slot: hid.at[slot, i]

    def hid_sem(sems, i):
        return lambda k: sems.at[i, k]

    def hid_args(i):
        return hid_view(i), hid_sem(hs, i), hid_sem(hr, i)

    def consume(i, carry):
        for w in range(2):
            for k in range(1, n):
                weight_copy(w, k, 0, i, origin[k]).wait_recv()
        w_all = jnp.concatenate(
            [gout[pl.ds(i * group, group)].reshape(gl, d), uout[pl.ds(i * group, group)].reshape(gl, d)], axis=0
        )

        def rows_step(r, c):
            rs = at(r * block, block)
            h = silu_mul(nt_dot(x[rs, :], w_all), inv[rs, :gl])
            lane = lax.broadcasted_iota(jnp.int32, h.shape, 1)
            expert = (me * le + group * i + lane // hl).astype(jnp.float32)
            weight = jnp.zeros(h.shape, jnp.float32)
            for k in range(topk):
                weight = weight + jnp.where(
                    routes[rs, k : k + 1] == expert, routes[rs, topk + k : topk + k + 1], 0.0
                )
            hid[tp, i, rs, :] = (h * weight).astype(jnp.bfloat16)
            return c

        if total_rows == block:
            rows_step(0, 0)
        else:
            lax.fori_loop(0, total_rows // block, rows_step, 0)

        @pl.when(i > 0)
        def _():
            z_relay(*hid_args(i - 1))

        z_send(*hid_args(i))

        if pairs > slots:

            @pl.when(i == pairs - slots - 1)
            def _():
                for q in range(2):
                    gather_relay(small_place(q), small_sems[q])

        @pl.when(i + slots < pairs)
        def _():
            for w in range(2):
                for k in range(1, n):
                    weight_copy(w, k, lax.rem(i, slots), i, me).wait_send()
            produce(i + slots)

        if pairs > slots:

            @pl.when(i == pairs - slots - 1)
            def _():
                produce_down()

        return carry

    if pairs == slots:
        for q in range(2):
            gather_relay(small_place(q), small_sems[q])
        produce_down()
    lax.fori_loop(0, pairs, consume, 0)
    z_relay(*hid_args(pairs - 1))

    for i in range(2):
        gather_wait(small_place(i), small_sems[i])
    shared_all = jnp.concatenate([sgo[...], suo[...]], axis=0)

    def shared_step(r, c):
        rs = at(r * block, block)
        h = silu_mul(nt_dot(x[rs, :], shared_all), inv[rs, :hl])
        wide = jnp.concatenate([h] * group, axis=1)
        lane = lax.broadcasted_iota(jnp.int32, wide.shape, 1)
        hid[tp, pairs, rs, :] = jnp.where(lane // hl == lax.rem(tp, sources), wide, 0.0).astype(jnp.bfloat16)
        return c

    if total_rows == block:
        shared_step(0, 0)
    else:
        lax.fori_loop(0, total_rows // block, shared_step, 0)
    z_send(*hid_args(pairs))

    def finish(i, carry):
        z_finish(*hid_args(i))
        return carry

    lax.fori_loop(0, pairs, finish, 0)
    z_relay(*hid_args(pairs))
    z_finish(*hid_args(pairs))

    def part_copy(k, cb, who):
        return pltpu.make_async_remote_copy(
            src_ref=part.at[cb, at(who * rows, rows)],
            dst_ref=landed.at[cb, k - 1],
            send_sem=cs.at[cb, k - 1],
            recv_sem=cr.at[cb, k - 1],
            device_id=to_fs(k),
            device_id_type=MESH,
        )

    per = ge // group
    mine = at(me * rows, rows)

    def down_step(c, carry):
        cb, eg = c // neg, lax.rem(c, neg)
        for k in range(1, n):
            down_copy(k, c, origin[k]).wait_recv()
        left, right = [], []
        for p in range(per):
            pair = eg * per + p
            for s in range(ntp):
                left.append(hid.at[s, pair])
                right.append(
                    dout[pl.ds(pair * group, group), s * hl : (s + 1) * hl, at(cb * cw, cw)].reshape(gl, cw)
                )
        down = jnp.concatenate(right, axis=0)

        def rows_step(r, q):
            rs = at(r * block, block)
            lhs = jnp.concatenate([ref[rs, :] for ref in left], axis=1)
            total = jnp.dot(lhs, down, preferred_element_type=jnp.float32)

            @pl.when(eg == 0)
            def _():
                units = functools.reduce(jnp.add, [hid[me * sources + q, pairs, rs, :hd] for q in range(sources)])
                shared = jnp.dot(units, ssb[:, at(cb * cw, cw)], preferred_element_type=jnp.float32)
                acc[rs, :] = total + shared

            @pl.when(eg > 0)
            def _():
                acc[rs, :] += total

            return q

        if total_rows == block:
            rows_step(0, 0)
        else:
            lax.fori_loop(0, total_rows // block, rows_step, 0)

        if cols > 1:

            @pl.when((eg == neg - 1) & (cb < cols - 1))
            def _():
                part[cb] = acc[...].astype(jnp.bfloat16)
                own[:, at(cb * cw, cw)] = acc[mine, :]
                for k in range(1, n):
                    part_copy(k, cb, dest[k]).start()

        return carry

    lax.fori_loop(0, chunks, down_step, 0)
    fold = rows // cols
    for k in range(1, n):
        to = mate(me, turn(k, n), n)
        lasts[k - 1][:hd, :] = ssb[...]
        for c in range(cols):
            lasts[k - 1][hd:, c * cw : (c + 1) * cw] = acc[at(to * rows + c * fold, fold), :].astype(jnp.bfloat16)
    own[:, cl - cw :] = acc[mine, :]

    for k in range(1, n):
        route_copy(k, me).wait_send()
    gather_sent(token_place, token_sems)
    for i in range(2):
        gather_sent(small_place(i), small_sems[i])
    z_sent(token_view, pick(zs), pick(zr))

    def sent(i, carry):
        z_sent(*hid_args(i))
        return carry

    lax.fori_loop(0, pairs + 1, sent, 0)

    def weights_sent(j, carry):
        for w in range(2):
            for k in range(1, n):
                weight_copy(w, k, lax.rem(j, slots), j, me).wait_send()
        return carry

    lax.fori_loop(pairs - slots, pairs, weights_sent, 0)

    def down_sent(c, carry):
        for k in range(1, n):
            down_copy(k, c, me).wait_send()
        return carry

    lax.fori_loop(0, chunks, down_sent, 0)

    for cb in range(cols - 1):
        result = own[:, cb * cw : (cb + 1) * cw]
        for k in range(1, n):
            part_copy(k, cb, dest[k]).wait()
            result = result + landed[cb, k - 1].astype(jnp.float32)
        own[:, cb * cw : (cb + 1) * cw] = result


def moe_call(n, ntp, args):
    ids, aff, gain, tokens, gate, up, down, sg, su, sd = args
    bf16, f32 = jnp.bfloat16, jnp.float32
    experts, hl, dl = gate.shape
    _, hd, cl = down.shape
    rows = tokens.shape[0]
    topk = ids.shape[0]
    le, d, hidden, total = experts // n, dl * n, hd * n, rows * n
    group = min(le, max(1, 128 // hl))
    pairs = le // group
    slots = min(6, pairs)
    cols = 2 if cl % 256 == 0 else 1
    cw, early = cl // cols, max(1, cols - 1)
    ge = group * (2 if pairs % 2 == 0 else 1)
    chunks = cols * (le // ge)
    gl = group * hl
    nz = ntp // 2
    vm, dma = pltpu.VMEM, pltpu.SemaphoreType.DMA
    serve = [((le, hl, d), bf16), ((le, hl, d), bf16), ((le, hidden, cl), bf16), ((hl, d), bf16), ((hl, d), bf16)]
    outs = serve + [((rows, cl), f32)] + [((hd + rows // cols, cl), bf16)] * (n - 1)
    pinned = sum(functools.reduce(lambda a, b: a * b, s) * jnp.dtype(t).itemsize for s, t in outs)
    hbm = pl.BlockSpec(memory_space=pltpu.HBM)
    args = [pltpu.with_memory_space_constraint(a, pltpu.HBM) for a in args]
    results = pl.pallas_call(
        functools.partial(moe_kernel, (n, ntp, group, slots, cols, ge)),
        out_shape=tuple(vm(s, t) for s, t in outs),
        in_specs=[hbm] * len(args),
        out_specs=(pl.BlockSpec(memory_space=vm),) * len(outs),
        scratch_shapes=[
            vm(ids.shape, ids.dtype),
            vm(aff.shape, f32),
            vm(gain.shape, f32),
            vm((2 * topk, rows), f32),
            vm((n, 2 * topk, rows), f32),
            vm((total, 128), f32),
            vm((total, d), bf16),
            vm((total, 128), f32),
            vm((n, group, hl, dl), f32),
            vm((2, n - 1, slots, group, hl, dl), bf16),
            vm((n, ge, hd, cw), f32),
            vm((n - 1, chunks, ge, hd, cw), bf16),
            vm(sg.shape, f32),
            vm(su.shape, f32),
            vm(sd.shape, f32),
            vm(sd.shape, bf16),
            vm((ntp, pairs + 1, total, gl), bf16),
            vm((total, cw), f32),
            vm((early, total, cw), bf16),
            vm((early, n - 1, rows, cw), bf16),
            dma((6,)),
            dma((2, n)),
            dma((2, max(4, n))),
            dma,
            dma((2 * nz - 1,)),
            dma((2 * nz - 1,)),
            dma((2, n - 1, slots)),
            dma((2, n - 1, pairs)),
            dma((n - 1, chunks)),
            dma((n - 1, chunks)),
            dma((2, max(4, n))),
            dma((2, max(4, n))),
            dma((pairs + 1, 2 * nz - 1)),
            dma((pairs + 1, 2 * nz - 1)),
            dma((early, n - 1)),
            dma((early, n - 1)),
            dma((2, n)),
        ],
        compiler_params=pltpu.CompilerParams(
            collective_id=0, has_side_effects=True, vmem_limit_bytes=min(60 * 1024 * 1024, vmem_bytes - pinned)
        ),
        cost_estimate=pl.CostEstimate(flops=6 * total * d * hl * le, bytes_accessed=40 * gate.size, transcendentals=0),
    )(*args)

    cut = 1

    def write(*refs):
        count = len(serve)
        sem = refs[-1]
        copies = []
        for i in range(count):
            step = refs[i].shape[0] // cut
            for c in range(cut):
                piece = pl.ds(c * step, step)
                copies.append(pltpu.make_async_copy(refs[i].at[piece], refs[count + i].at[piece], sem.at[i, c]))
        for c in copies:
            c.start()
        for c in copies:
            c.wait()

    own, sent = results[len(serve)], results[len(serve) + 1 :]
    moved = [lax.ppermute(sent[k - 1], "fs", mate_pairs(turn(k, n), n)) for k in range(1, n)]
    written = pl.pallas_call(
        write,
        out_shape=tuple(jax.ShapeDtypeStruct(s, t) for s, t in serve),
        in_specs=[pl.BlockSpec(memory_space=vm)] * len(serve),
        out_specs=(hbm,) * len(serve),
        scratch_shapes=[dma((len(serve), cut))],
        compiler_params=pltpu.CompilerParams(vmem_limit_bytes=1024 * 1024),
        cost_estimate=pl.CostEstimate(flops=0, bytes_accessed=10 * pinned, transcendentals=0),
    )(*results[: len(serve)])
    mixed, shared_down = finish_call(n, hd, own, sent[0], moved)
    return (mixed, *written, shared_down)


def finish_kernel(n, hd, own, *refs):
    pieces = refs[:n]
    mixed_ref, down_ref, sem = refs[n:]
    me = lax.axis_index("fs")
    copies = []
    for k in range(n):
        source = mate_origin(me, turn(k, n), n)
        place = down_ref.at[pl.ds(pl.multiple_of(source * hd, hd), hd)]
        copies.append(pltpu.make_async_copy(pieces[k].at[pl.ds(0, hd)], place, sem.at[k]))
        copies[-1].start()
    rows, cl = own.shape
    fold = pieces[0].shape[0] - hd
    cols = rows // fold
    cw = cl // cols
    early = cl - cw
    if early:
        mixed_ref[:, :early] = own[:, :early].astype(mixed_ref.dtype)
    for c in range(cols):
        part = slice(c * fold, (c + 1) * fold)
        total = own[part, early:]
        for k in range(1, n):
            total = total + pieces[k][hd:, c * cw : (c + 1) * cw].astype(jnp.float32)
        mixed_ref[part, early:] = total.astype(mixed_ref.dtype)
    for c in copies:
        c.wait()


def finish_call(n, hd, own, sent, moved):
    vmem = pl.BlockSpec(memory_space=pltpu.VMEM)
    return pl.pallas_call(
        functools.partial(finish_kernel, n, hd),
        out_shape=(
            jax.ShapeDtypeStruct(own.shape, jnp.bfloat16),
            jax.ShapeDtypeStruct((n * hd, own.shape[1]), jnp.bfloat16),
        ),
        in_specs=[vmem] * (n + 1),
        out_specs=(vmem, pl.BlockSpec(memory_space=pltpu.HBM)),
        scratch_shapes=[pltpu.SemaphoreType.DMA((n,))],
        compiler_params=pltpu.CompilerParams(vmem_limit_bytes=4 * 1024 * 1024),
    )(own, sent, *moved)


def body(
    n,
    ntp,
    tokens,
    expert_ids,
    affinity,
    norm_gain,
    gate_train,
    up_train,
    down_train,
    shared_gate_train,
    shared_up_train,
    shared_down_train,
):
    return moe_call(
        n,
        ntp,
        [
            expert_ids.T,
            affinity.T,
            norm_gain[None, :],
            tokens,
            gate_train,
            up_train,
            down_train,
            shared_gate_train,
            shared_up_train,
            shared_down_train,
        ],
    )


def solution(mesh):
    return jax.shard_map(
        functools.partial(body, mesh.shape["fs"], mesh.shape["tp"]),
        mesh=mesh,
        in_specs=(
            P("fs", "tp"),
            P("fs", None),
            P("fs", None),
            P("fs"),
            P(None, "tp", "fs"),
            P(None, "tp", "fs"),
            P(None, "fs", "tp"),
            P("tp", "fs"),
            P("tp", "fs"),
            P("fs", "tp"),
        ),
        out_specs=(
            P("fs", "tp"),
            P("fs", "tp", None),
            P("fs", "tp", None),
            P("fs", None, "tp"),
            P("tp", None),
            P("tp", None),
            P(None, "tp"),
        ),
        check_vma=False,
    )
```
